32 devices in a mesh: sp: 8 (over z, y), tp: 4 (over x, core).
Axes of the slice: x: 2, y: 2, z: 4, core: 2. Of those that a mesh axis runs over, the one named last changes fastest.
Arguments:
- query_rows: bfloat16 [4096, 2048], P('sp', 'tp'), may hold values from -40 to 40
- key_rows: bfloat16 [4096, 256], P('sp', 'tp'), may hold values from -6 to 6
- value_rows: bfloat16 [4096, 256], P('sp', 'tp'), may hold values from -12 to 12
- doc_ids: int32 [4096], P('sp'), may hold values from 0 to 3, never falling along the last dimension, each value on 1 to 2048 neighbouring positions
- sink_logit: float32 [32], P('tp'), may hold values from 1 to 6
- residual: bfloat16 [4096, 2048], P('sp'), may hold values from -10 to 10
- out_proj: bfloat16 [2048, 2048], P('tp'), may hold values from -0.25 to 0.25
- mix_gain: float32 [2048], replicated, may hold values from 0.1 to 1.9
- gate_proj: bfloat16 [2048, 5632], P('sp', 'tp'), may hold values from -0.125 to 0.125
- value_proj: bfloat16 [2048, 5632], P('sp', 'tp'), may hold values from -0.125 to 0.125
- gate_taps: float32 [3, 5632], P(None, 'tp'), may hold values from -3 to 3
- value_taps: float32 [3, 5632], P(None, 'tp'), may hold values from -3 to 3
- down_proj: bfloat16 [5632, 2048], P('tp', 'sp'), may hold values from -0.078125 to 0.078125
- final_gain: float32 [2048], P('tp'), may hold values from 0.1 to 1.9
Outputs:
- mixed: bfloat16 [4096, 2048], P('sp', 'tp')
The draws below stay inside these ranges and needn't reach their ends.
All inputs are finite; a program needn't handle non-finite values.
Results may differ from the reference program's by a relative error of at most 0.012.
Values may be sent and summed in bfloat16 or wider, within the bound.
No kernel may reach another device: no remote copies, remote signals or barrier semaphores. Data moves between devices by JAX's collectives and lax.ppermute only.
A program may use at most 128 MiB of HBM per device.

```python
import math
import jax
import jax.numpy as jnp
import numpy as np
from jax import lax

D = 2048
HQ = 32
HK = 4
HD = 64
FF = 5632
WIN = 128
TAPS = 3
TOK_DEV = 512
TOKENS = 4096
DOC_COUNT = 4
DOC_MOST = 2048
N_TP = 4


def draw_key_rows(key, part):
    drawn = jax.random.truncated_normal(jax.random.fold_in(key, 1), -6.0, 6.0, (TOKENS, HK, HD), jnp.float32)
    return drawn.reshape(TOKENS, HK * HD).astype(jnp.bfloat16)


def draw_query_rows(key, part):
    drawn = jax.random.truncated_normal(jax.random.fold_in(key, 3), -6.0, 6.0, (TOKENS, HQ, HD), jnp.float32)
    return drawn.reshape(TOKENS, HQ * HD).astype(jnp.bfloat16)


def draw_residual(key, part):
    columns = jnp.arange(D, dtype=jnp.float32) / max(D - 1, 1)
    base = 0.4 * jax.random.truncated_normal(key, -6.0, 6.0, (TOKENS, D), jnp.float32)
    scale = jnp.exp(columns * math.log(4.0))
    return (base * scale[None, :]).astype(jnp.bfloat16)


def levels(stream_key, shape, pieces, smallest, largest):
    level, own = 1.0, jax.random.fold_in(stream_key, 6)
    for position, shards_of in pieces:
        steps = jnp.exp(jax.random.uniform(jax.random.fold_in(own, position), (shards_of,), jnp.float32, smallest / len(pieces), largest / len(pieces)))
        level = level * jnp.repeat(steps, shape[position] // shards_of).reshape([-1 if axis == position else 1 for axis in range(len(shape))])
    return level


def split_up(number_of, total, reach, skew):
    loads = [(1 << 20) // math.isqrt(standing ** skew) + 1 for standing in range(2, number_of + 1)]
    rest, holding = total - reach - (number_of - 1), [1] * (number_of - 1)
    while rest > 0:
        candidates = [i for i in range(number_of - 1) if holding[i] < reach]
        whole, left = sum([loads[i] for i in candidates]), rest
        for i in candidates:
            extra = min(reach - holding[i], max(1, left * loads[i] // whole), rest)
            holding[i] = holding[i] + extra
            rest = rest - extra
    return np.array([reach] + holding)


def uneven_parts(stream_key, count, total, most, slope):
    if count == 2:
        one = jax.random.randint(stream_key, (), max(1, total - most), min(most, total - 1) + 1)
        return jnp.stack([one, total - one])
    tallies = jnp.asarray(split_up(count, total, most, slope), jnp.int32)
    couples = (count - 1) // 2
    source_of, receiver = tallies[1:1 + 2 * couples:2], tallies[2:2 + 2 * couples:2]
    slack = jnp.minimum(source_of - 1, most - receiver)
    moved = jax.random.randint(jax.random.fold_in(stream_key, 1), (couples,), 0, 1 << 20) % (slack + 1)
    tallies = tallies.at[1:1 + 2 * couples:2].set(source_of - moved).at[2:2 + 2 * couples:2].set(receiver + moved)
    return tallies[jax.random.permutation(jax.random.fold_in(stream_key, 2), count)]


def noise(key, dims, scale, limit, pieces=(), kind=jnp.bfloat16):
    result = scale * jax.random.normal(key, dims, jnp.float32)
    if pieces:
        result = result * levels(key, dims, pieces, -0.22, 0.18)
    return jnp.clip(result, -limit, limit).astype(kind)


def setup_inputs(seed: int = 0) -> dict:
    arg_keys = jax.random.split(jax.random.key(seed), 15)
    return {
        "query_rows": draw_query_rows(jax.random.fold_in(arg_keys[14], 71), 0),
        "key_rows": draw_key_rows(jax.random.fold_in(arg_keys[14], 71), 0),
        "value_rows": noise(arg_keys[2], (TOKENS, HK * HD), 2.0, 12.0, ((0, 8), (1, 4))),
        "doc_ids": jnp.searchsorted(jnp.cumsum(uneven_parts(arg_keys[3], DOC_COUNT, TOKENS, DOC_MOST, 2)), jnp.arange(TOKENS), side="right").astype(jnp.int32),
        "sink_logit": jnp.clip(1.0 + 5.0 * jax.random.uniform(arg_keys[4], (HQ,), jnp.float32) ** levels(arg_keys[4], (HQ,), ((0, 4),), -0.2, 0.2), 1.0, 6.0),
        "residual": draw_residual(jax.random.fold_in(arg_keys[14], 71), 0),
        "out_proj": noise(arg_keys[6], (HQ * HD, D), (HQ * HD // 4) ** -0.5, 0.25, ((0, 4),)),
        "mix_gain": jnp.clip(1.0 + 0.18 * jax.random.normal(arg_keys[7], (D,), jnp.float32), 0.1, 1.9),
        "gate_proj": noise(arg_keys[8], (D, FF), D ** -0.5, 0.125, ((0, 8), (1, 4))),
        "value_proj": noise(arg_keys[9], (D, FF), D ** -0.5, 0.125, ((0, 8), (1, 4))),
        "gate_taps": noise(arg_keys[10], (TAPS, FF), 0.6, 3.0, ((1, 4),), jnp.float32),
        "value_taps": noise(arg_keys[11], (TAPS, FF), 0.6, 3.0, ((1, 4),), jnp.float32),
        "down_proj": noise(arg_keys[12], (FF, D), FF ** -0.5, 0.078125, ((0, 4), (1, 8))),
        "final_gain": jnp.clip(1.0 + 0.18 * jax.random.normal(arg_keys[13], (D,), jnp.float32), 0.1, 1.9),
    }


mix_scale = math.sqrt(2.0)
norm_eps = 1e-05

def attend(query_block, key_block, value_block, query_pos, key_pos, query_doc, key_doc, sink):
    head_size = query_block.shape[-1]
    scores = jnp.einsum('qkgd,skd->kgqs', query_block.astype(jnp.float32), key_block.astype(jnp.float32)) * head_size ** (-0.5)
    diff = query_pos[:, None] - key_pos[None, :]
    valid = (diff >= 0) & (diff < WIN) & (query_doc[:, None] == key_doc[None, :]) & (key_pos[None, :] >= 0)
    scores = jnp.where(valid[None, None], scores, -1e+30)
    top = jnp.maximum(lax.optimization_barrier(jnp.max(scores, axis=-1, keepdims=True)), sink)
    weights = jnp.exp(scores - top)
    total = lax.optimization_barrier(jnp.sum(weights, axis=-1, keepdims=True)) + jnp.exp(sink - top)
    probs = (weights / total).astype(jnp.bfloat16)
    out = jnp.einsum('kgqs,skd->qkgd', probs.astype(jnp.float32), value_block.astype(jnp.float32))
    return out.astype(jnp.bfloat16)

def depthwise(tail, current, taps, tail_docs, docs):
    extended = jnp.concatenate([tail, current])
    ext_docs = jnp.concatenate([tail_docs, docs])
    lag_rows = tail.shape[0]
    count = current.shape[0]
    total = jnp.zeros(current.shape, jnp.float32)
    for lag in range(lag_rows + 1):
        start = lag_rows - lag
        same = (ext_docs[start:start + count] == docs)[:, None]
        rows = extended[start:start + count].astype(jnp.float32)
        total = total + taps[lag].astype(jnp.float32)[None, :] * jnp.where(same, rows, 0.0)
    return total

def layer_norm(values, gain):
    mean = lax.optimization_barrier(jnp.mean(values, axis=1, keepdims=True))
    var = lax.optimization_barrier(jnp.mean(jnp.square(values - mean), axis=1, keepdims=True))
    return (values - mean) * lax.rsqrt(var + norm_eps) * gain.astype(jnp.float32)[None, :]

def reference(query_rows, key_rows, value_rows, doc_ids, sink_logit, residual, out_proj, mix_gain, gate_proj, value_proj, gate_taps, value_taps, down_proj, final_gain):
    groups = HQ // HK
    block = min(512, TOK_DEV)
    count = TOKENS // block
    queries = query_rows.reshape(TOKENS, HK, groups, HD)
    pad_keys = jnp.concatenate([jnp.zeros((WIN, HK * HD), jnp.bfloat16), key_rows]).reshape(TOKENS + WIN, HK, HD)
    pad_values = jnp.concatenate([jnp.zeros((WIN, HK * HD), jnp.bfloat16), value_rows]).reshape(TOKENS + WIN, HK, HD)
    docs = doc_ids.astype(jnp.int32)
    pad_docs = jnp.concatenate([jnp.full((WIN,), -1, jnp.int32), docs])
    sink = sink_logit.astype(jnp.float32).reshape(HK, groups, 1, 1)

    def one_block(index):
        start = (index * block).astype(jnp.int32)
        query_block = lax.dynamic_slice_in_dim(queries, start, block, 0)
        key_block = lax.dynamic_slice_in_dim(pad_keys, start, block + WIN, 0)
        value_block = lax.dynamic_slice_in_dim(pad_values, start, block + WIN, 0)
        query_doc = lax.dynamic_slice_in_dim(docs, start, block, 0)
        key_doc = lax.dynamic_slice_in_dim(pad_docs, start, block + WIN, 0)
        query_pos = start + jnp.arange(block, dtype=jnp.int32)
        key_pos = start - WIN + jnp.arange(block + WIN, dtype=jnp.int32)
        return attend(query_block, key_block, value_block, query_pos, key_pos, query_doc, key_doc, sink)
    heads = lax.map(one_block, jnp.arange(count, dtype=jnp.int32)).reshape(TOKENS, HQ * HD)
    head_cols = HQ * HD // N_TP
    attn_proj = jnp.zeros((TOKENS, D), jnp.float32)
    for group in range(N_TP):
        part = jnp.dot(heads[:, group * head_cols:(group + 1) * head_cols], out_proj[group * head_cols:(group + 1) * head_cols], preferred_element_type=jnp.float32)
        attn_proj = attn_proj + part.astype(jnp.bfloat16).astype(jnp.float32)
    first_sum = mix_scale * residual.astype(jnp.float32) + attn_proj
    normed = layer_norm(first_sum, mix_gain).astype(jnp.bfloat16)
    up_gate = jnp.dot(normed, gate_proj, preferred_element_type=jnp.float32).astype(jnp.bfloat16)
    up_value = jnp.dot(normed, value_proj, preferred_element_type=jnp.float32).astype(jnp.bfloat16)
    lag_rows = TAPS - 1
    zero_tail = jnp.zeros((lag_rows, FF), jnp.bfloat16)
    tail_docs = jnp.full((lag_rows,), -1, jnp.int32)
    conv_gate = depthwise(zero_tail, up_gate, gate_taps, tail_docs, docs)
    conv_value = depthwise(zero_tail, up_value, value_taps, tail_docs, docs)
    hidden = (jax.nn.gelu(conv_gate) * conv_value).astype(jnp.bfloat16)
    unit_cols = FF // N_TP
    ffn = jnp.zeros((TOKENS, D), jnp.float32)
    for group in range(N_TP):
        part = jnp.dot(hidden[:, group * unit_cols:(group + 1) * unit_cols], down_proj[group * unit_cols:(group + 1) * unit_cols], preferred_element_type=jnp.float32)
        ffn = ffn + part.astype(jnp.bfloat16).astype(jnp.float32)
    second_sum = mix_scale * normed.astype(jnp.float32) + ffn
    return layer_norm(second_sum, final_gain).astype(jnp.bfloat16)
```

```python
import functools
import math

import jax
import jax.numpy as jnp
from jax import lax
from jax.experimental import pallas as pl
from jax.experimental.pallas import tpu as pltpu
from jax.sharding import PartitionSpec as P


HD = 64
WIN = 128
TAPS = 3
LANES = 128
TAIL = 8


mix_scale = math.sqrt(2.0)
norm_eps = 1e-05


def passed_along(block, axis, distance):
    devices = range(lax.axis_size(axis))
    route = [(i - distance, i) for i in devices if i - distance in devices]
    return lax.ppermute(block, axis, route)


def swapped(block, sp_mask=0, tp_mask=0):
    n_sp, n_tp = lax.axis_size("sp"), lax.axis_size("tp")
    if not tp_mask:
        return lax.ppermute(block, "sp", [(i, i ^ sp_mask) for i in range(n_sp)])
    if not sp_mask:
        return lax.ppermute(block, "tp", [(i, i ^ tp_mask) for i in range(n_tp)])
    route = [
        (i * n_tp + j, (i ^ sp_mask) * n_tp + (j ^ tp_mask))
        for i in range(n_sp)
        for j in range(n_tp)
    ]
    return lax.ppermute(block, ("sp", "tp"), route)


def attend(query_block, key_block, value_block, query_pos, key_pos, query_doc, key_doc, sink):
    head_size = query_block.shape[-1]
    scores = jnp.einsum(
        "qkgd,skd->kgqs", query_block, key_block, preferred_element_type=jnp.float32
    ) * head_size ** (-0.5)
    diff = query_pos[:, None] - key_pos[None, :]
    valid = (
        (diff >= 0)
        & (diff < WIN)
        & (query_doc[:, None] == key_doc[None, :])
        & (key_pos[None, :] >= 0)
    )
    scores = jnp.where(valid[None, None], scores, -1e30)
    top = jnp.maximum(jnp.max(scores, axis=-1, keepdims=True), sink)
    weights = jnp.exp(scores - top)
    total = jnp.sum(weights, axis=-1, keepdims=True) + jnp.exp(sink - top)
    probs = (weights / total).astype(jnp.bfloat16)
    out = jnp.einsum("kgqs,skd->qkgd", probs, value_block, preferred_element_type=jnp.float32)
    return out.astype(jnp.bfloat16)


def depthwise(tail, current, taps, tail_docs, docs):
    extended = jnp.concatenate([tail, current])
    ext_docs = jnp.concatenate([tail_docs, docs])
    lag_rows = tail.shape[0]
    count = current.shape[0]
    total = jnp.zeros(current.shape, jnp.float32)
    for lag in range(lag_rows + 1):
        start = lag_rows - lag
        same = (ext_docs[start : start + count] == docs)[:, None]
        rows = extended[start : start + count].astype(jnp.float32)
        total = total + taps[lag][None, :] * jnp.where(same, rows, 0.0)
    return total


def room(mib):
    return pltpu.CompilerParams(vmem_limit_bytes=mib << 20)


def hbm():
    return pl.BlockSpec(memory_space=pltpu.HBM)


def vmem():
    return pl.BlockSpec(memory_space=pltpu.VMEM)


def prepare_kernel(
    which, gates, values_in, queries, keys, values, docs, residual, own, other, halo, *scratch
):
    q, k, v, r, gate, value, sems = scratch
    cols = gate.shape[1]
    rows = queries.shape[0]
    whole = [
        pltpu.make_async_copy(src, dst, sems.at[4 + i])
        for i, (src, dst) in enumerate(((gates, gate), (values_in, value)))
    ]
    for copy in whole:
        copy.start()
    copies = [
        pltpu.make_async_copy(src.at[pl.ds(rows - TAIL, TAIL)], dst, sems.at[i])
        for i, (src, dst) in enumerate(((queries, q), (residual, r)))
    ] + [
        pltpu.make_async_copy(src.at[:, pl.ds(rows - 2 * WIN, 2 * WIN)], dst, sems.at[2 + i])
        for i, (src, dst) in enumerate(((keys, k), (values, v)))
    ]
    for copy in copies:
        copy.start()
    for copy in copies:
        copy.wait()
    at = 0
    for src in (k, v, docs, q, r):
        for n in range(0, src.shape[1], LANES):
            halo[at : at + src.shape[0], :] = src[:, n : n + LANES]
            at += src.shape[0]
    for copy in whole:
        copy.wait()
    half = cols // 2
    main = half // LANES * LANES
    rest = half - main

    def emit(part, out):
        start = part * (cols - main)
        for n in range(0, main, LANES):
            out[:, 2 * n : 2 * n + LANES] = gate[:, start + n : start + n + LANES]
            out[:, 2 * n + LANES : 2 * n + 2 * LANES] = value[:, start + n : start + n + LANES]
        left = gate[:, main : main + LANES].astype(jnp.float32)
        right = value[:, main : main + LANES].astype(jnp.float32)
        if part:
            left = pltpu.roll(left, rest, 1)
        else:
            right = pltpu.roll(right, rest, 1)
        lane = lax.broadcasted_iota(jnp.int32, left.shape, 1)
        out[:, 2 * main :] = jnp.where(lane < rest, left, right).astype(out.dtype)

    @pl.when(which[0] == 0)
    def _():
        emit(0, own)
        emit(1, other)

    @pl.when(which[0] != 0)
    def _():
        emit(1, own)
        emit(0, other)


def prepared(which, gate, value, queries, keys, values, docs, residual):
    shape = jax.ShapeDtypeStruct(gate.shape, gate.dtype)
    lines = 4 * HD * WIN // LANES + TAIL + TAIL * (queries.shape[1] + residual.shape[1]) // LANES
    scratch = [(TAIL, queries.shape[1]), (HD, 2 * WIN), (HD, 2 * WIN)]
    scratch += [(TAIL, residual.shape[1]), gate.shape, gate.shape]
    return pl.pallas_call(
        prepare_kernel,
        in_specs=[pl.BlockSpec(memory_space=pltpu.SMEM)] + [hbm()] * 5 + [vmem(), hbm()],
        out_specs=[vmem()] * 3,
        out_shape=[shape, shape, jax.ShapeDtypeStruct((lines, LANES), jnp.bfloat16)],
        scratch_shapes=[pltpu.VMEM(size, jnp.bfloat16) for size in scratch]
        + [pltpu.SemaphoreType.DMA((6,))],
        compiler_params=room(56),
        name="prepare",
    )(which, gate, value, queries, keys.T, values.T, docs, residual)


def row_halves_kernel(which, down, own, other, sems):
    rows = down.shape[0]
    half = rows // 2
    main = half // LANES * LANES
    rest = half - main
    for f, out in enumerate((own, other)):
        part = which[0] ^ f
        start = pl.multiple_of(part * (rows - main), 2 * TAIL)
        left = pl.multiple_of(main + part * rest, 2 * TAIL)
        copies = [
            pltpu.make_async_copy(
                down.at[pl.ds(start, main)], out.at[pl.ds(0, main)], sems.at[f, 0]
            ),
            pltpu.make_async_copy(
                down.at[pl.ds(left, rest)], out.at[pl.ds(main, rest)], sems.at[f, 1]
            ),
        ]
        for copy in copies:
            copy.start()
    for f, out in enumerate((own, other)):
        pltpu.make_async_copy(
            down.at[pl.ds(0, main)], out.at[pl.ds(0, main)], sems.at[f, 0]
        ).wait()
        pltpu.make_async_copy(
            down.at[pl.ds(0, rest)], out.at[pl.ds(main, rest)], sems.at[f, 1]
        ).wait()


def row_halves(which, down):
    shape = jax.ShapeDtypeStruct((down.shape[0] // 2, down.shape[1]), down.dtype)
    return pl.pallas_call(
        row_halves_kernel,
        in_specs=[pl.BlockSpec(memory_space=pltpu.SMEM), hbm()],
        out_specs=[vmem(), vmem()],
        out_shape=[shape, shape],
        scratch_shapes=[pltpu.SemaphoreType.DMA((2, 2))],
        compiler_params=room(56),
        name="row_halves",
    )(which, down)


def up_kernel(place, *refs, pieces, quarter):
    chunks = refs[:4]
    weights = refs[4 : 4 + pieces]
    taps, hidden, own_normed, xs, ws, up, flags, same, sems = refs[4 + pieces :]
    sp, tp = place[0], place[1]
    x, core = tp // 2, tp % 2
    piece_rows = weights[0].shape[0]
    block = 4 * quarter
    copies = []

    def begin(src, dst):
        copy = pltpu.make_async_copy(src, dst, sems.at[len(copies)])
        copy.start()
        copies.append(copy)

    for i, chunk in enumerate(chunks):
        number = (x ^ (i % 2)) * 2 + (core ^ (i // 2))
        begin(
            chunk.at[pl.ds(TAIL, quarter)],
            xs.at[pl.ds(pl.multiple_of(TAIL + number * quarter, TAIL), quarter)],
        )

        begin(chunk.at[pl.ds(0, TAIL), pl.ds(0, LANES)], flags.at[number])

        @pl.when(number == 0)
        def _(chunk=chunk):
            pltpu.make_async_copy(
                chunk.at[pl.ds(0, TAIL)], xs.at[pl.ds(0, TAIL)], sems.at[8 + pieces]
            ).start()

    for j in range(pieces):
        begin(weights[j], ws.at[pl.ds(pl.multiple_of((sp ^ j) * piece_rows, piece_rows), piece_rows)])
    pltpu.make_async_copy(
        chunks[0].at[pl.ds(0, TAIL)], xs.at[pl.ds(0, TAIL)], sems.at[8 + pieces]
    ).wait()
    for copy in copies:
        copy.wait()

    half = ws.shape[1] // 2
    main = half // LANES * LANES
    rest = half - main
    pair = 2 * LANES
    sub = 64
    line = lax.broadcasted_iota(jnp.int32, (quarter, quarter), 0)
    diagonal = line == lax.broadcasted_iota(jnp.int32, (quarter, quarter), 1)
    ones = jnp.ones((quarter, LANES), jnp.bfloat16)
    for i in range(4):
        rows = flags[i].astype(jnp.float32)
        for lag in range(2):
            spread = jnp.where(diagonal, rows[lag : lag + 1], 0.0).astype(jnp.bfloat16)
            same[lag, i * quarter : (i + 1) * quarter] = jnp.dot(
                spread, ones, preferred_element_type=jnp.float32
            )
    up[...] = jnp.dot(xs[...], ws[...], preferred_element_type=jnp.float32)

    def conv(rows, start, tap, one, two):
        lag1 = rows[TAIL - 1 : TAIL - 1 + sub, start : start + LANES]
        lag2 = rows[TAIL - 2 : TAIL - 2 + sub, start : start + LANES]
        return (
            tap[0:1] * rows[TAIL:, start : start + LANES]
            + tap[1:2] * jnp.where(one > 0, lag1, 0.0)
            + tap[2:3] * jnp.where(two > 0, lag2, 0.0)
        )

    def gelu(v):
        inner = v * (math.sqrt(2.0 / math.pi) + (0.044715 * math.sqrt(2.0 / math.pi)) * (v * v))
        return (0.5 * v) * (1.0 + jnp.tanh(inner))

    def mix(i, _):
        at = pl.ds(pl.multiple_of(i * sub, sub), sub)
        reach = pl.ds(pl.multiple_of(i * sub, sub), sub + TAIL)
        one, two = same[0, at, :], same[1, at, :]
        for n in range(0, main, LANES):
            rows = up[reach, 2 * n : 2 * n + pair]
            tap = taps[:, 2 * n : 2 * n + pair]
            h = gelu(conv(rows, 0, tap[:, :LANES], one, two))
            h = h * conv(rows, LANES, tap[:, LANES:], one, two)
            hidden[at, n : n + LANES] = h.astype(hidden.dtype)
        mixed = conv(up[reach, 2 * main :], 0, taps[:, 2 * main :], one, two)
        h = gelu(mixed) * pltpu.roll(mixed, rest, 1)
        hidden[at, main:] = h[:, :rest].astype(hidden.dtype)
        return 0

    lax.fori_loop(0, block // sub, mix, 0)
    share = own_normed.shape[1]
    own_normed[...] = xs[TAIL:, pl.ds(pl.multiple_of(tp * share, share), share)]


def up_hidden(place, chunks, weights, taps, share):
    quarter = chunks[0].shape[0] - TAIL
    width = chunks[0].shape[1]
    block = 4 * quarter
    cols = weights[0].shape[1]
    anywhere = pl.BlockSpec(memory_space=pl.ANY)
    return pl.pallas_call(
        functools.partial(up_kernel, pieces=len(weights), quarter=quarter),
        in_specs=[pl.BlockSpec(memory_space=pltpu.SMEM)]
        + [anywhere] * (4 + len(weights))
        + [vmem()],
        out_specs=[vmem(), vmem()],
        out_shape=[
            jax.ShapeDtypeStruct((block, cols // 2), jnp.bfloat16),
            jax.ShapeDtypeStruct((block, share), jnp.bfloat16),
        ],
        scratch_shapes=[
            pltpu.VMEM((block + TAIL, width), jnp.bfloat16),
            pltpu.VMEM((width, cols), jnp.bfloat16),
            pltpu.VMEM((block + TAIL, cols), jnp.float32),
            pltpu.VMEM((4, TAIL, LANES), jnp.bfloat16),
            pltpu.VMEM((2, block, LANES), jnp.float32),
            pltpu.SemaphoreType.DMA((9 + len(weights),)),
        ],
        compiler_params=room(24),
        name="up_hidden",
    )(place, *chunks, *weights, taps)


def project_kernel(place, heads, weights, keep, send, left, right, made, came, went, *, quarter):
    core = place[1] % 2
    count = right.shape[0]
    wide = right.shape[2]
    loads = [pltpu.make_async_copy(heads, left, came.at[count])]
    for n in range(count):
        cols = pl.ds(n * wide, wide)
        loads.append(pltpu.make_async_copy(weights.at[:, cols], right.at[n], came.at[n]))
    for copy in loads:
        copy.start()
    loads[0].wait()
    stores = []
    for n in range(count):
        loads[1 + n].wait()
        term = jnp.dot(left[...], right[n], preferred_element_type=jnp.float32)
        made[n] = term.astype(made.dtype)
        for f, (out, owner) in enumerate(((send, 1 - core), (keep, core))):
            for x in range(2):
                start = pl.multiple_of((2 * x + owner) * quarter, quarter)
                copy = pltpu.make_async_copy(
                    made.at[n, pl.ds(start, quarter + TAIL)],
                    out.at[x, :, pl.ds(n * wide, wide)],
                    went.at[n, 2 * f + x],
                )
                copy.start()
                stores.append(copy)
    for copy in stores:
        copy.wait()


def project(place, heads, weights, quarter):
    count, rows = 4, heads.shape[0]
    depth, width = weights.shape
    shape = jax.ShapeDtypeStruct((2, quarter + TAIL, width), jnp.bfloat16)
    anywhere = pl.BlockSpec(memory_space=pl.ANY)
    return pl.pallas_call(
        functools.partial(project_kernel, quarter=quarter),
        in_specs=[pl.BlockSpec(memory_space=pltpu.SMEM), anywhere, anywhere],
        out_specs=[anywhere, anywhere],
        out_shape=[shape, shape],
        scratch_shapes=[
            pltpu.VMEM((rows, depth), jnp.bfloat16),
            pltpu.VMEM((count, depth, width // count), jnp.bfloat16),
            pltpu.VMEM((count, rows, width // count), jnp.bfloat16),
            pltpu.SemaphoreType.DMA((count + 1,)),
            pltpu.SemaphoreType.DMA((count, 4)),
        ],
        compiler_params=room(56),
        name="project",
    )(place, heads, weights)


def merge_kernel(which, first, second, keep, send, a, b, c, came, went, *, axis):
    own = which[0]
    pieces = []
    for out, part in ((send, 1 - own), (keep, own)):
        for j in range(first.shape[1 - axis]):
            pieces.append((out.at[j], (part, j) if axis == 0 else (j, part)))
    copies = []
    for i, (_, at) in enumerate(pieces):
        pair = [
            pltpu.make_async_copy(src.at[at], dst.at[i], came.at[i, f])
            for f, (src, dst) in enumerate(((first, a), (second, b)))
        ]
        for copy in pair:
            copy.start()
        copies.append(pair)
    outs = []
    for i, (out, _) in enumerate(pieces):
        for copy in copies[i]:
            copy.wait()
        c[i] = a[i] + b[i]
        outs.append(pltpu.make_async_copy(c.at[i], out, went.at[i]))
        outs[-1].start()
    for copy in outs:
        copy.wait()


def merge(which, first, second, axis, mib=8):
    count = first.shape[1 - axis]
    shape = jax.ShapeDtypeStruct((count, *first.shape[2:]), jnp.bfloat16)
    anywhere = pl.BlockSpec(memory_space=pl.ANY)
    scratch = pltpu.VMEM((2 * count, *first.shape[2:]), jnp.bfloat16)
    return pl.pallas_call(
        functools.partial(merge_kernel, axis=axis),
        in_specs=[pl.BlockSpec(memory_space=pltpu.SMEM), anywhere, anywhere],
        out_specs=[anywhere, anywhere],
        out_shape=[shape, shape],
        scratch_shapes=[scratch] * 3
        + [pltpu.SemaphoreType.DMA((2 * count, 2)), pltpu.SemaphoreType.DMA((2 * count,))],
        compiler_params=room(mib),
        name="merge",
    )(which, first, second)


def norm_kernel(place, first, second, residual, before, gain, flags, out, base, sems):
    tp = place[1]
    rows = first.shape[0]
    quarter = rows - TAIL
    start = pl.multiple_of(tp * quarter, quarter)
    body = pltpu.make_async_copy(
        residual.at[pl.ds(start, quarter)], base.at[pl.ds(TAIL, quarter)], sems.at[0]
    )
    body.start()
    top = base.at[pl.ds(0, TAIL)]

    @pl.when(tp == 0)
    def _():
        pltpu.make_async_copy(before, top, sems.at[1]).start()

    @pl.when(tp != 0)
    def _():
        at = pl.multiple_of(jnp.maximum(start - TAIL, 0), TAIL)
        pltpu.make_async_copy(residual.at[pl.ds(at, TAIL)], top, sems.at[1]).start()

    pltpu.make_async_copy(before, top, sems.at[1]).wait()
    body.wait()
    group = 64
    for r in range(0, rows, group):
        at = slice(r, min(r + group, rows))
        total = first[at].astype(jnp.float32) + second[at].astype(jnp.float32)
        total = mix_scale * base[at].astype(jnp.float32) + total
        mean = jnp.mean(total, axis=1, keepdims=True)
        var = jnp.mean(total * total, axis=1, keepdims=True) - mean * mean
        out[at] = ((total - mean) * lax.rsqrt(var + norm_eps) * gain[...]).astype(out.dtype)
    line = lax.broadcasted_iota(jnp.int32, (TAIL, LANES), 0)
    rows_of = out[:TAIL, :LANES].astype(jnp.float32)
    out[:TAIL, :LANES] = jnp.where(line < 2, flags[...], rows_of).astype(out.dtype)


def normed_rows(place, first, second, residual, before, gain, flags):
    return pl.pallas_call(
        norm_kernel,
        in_specs=[pl.BlockSpec(memory_space=pltpu.SMEM), vmem(), vmem(), hbm(), hbm(), vmem(), vmem()],
        out_specs=vmem(),
        out_shape=jax.ShapeDtypeStruct(first.shape, jnp.bfloat16),
        scratch_shapes=[pltpu.VMEM(first.shape, jnp.bfloat16), pltpu.SemaphoreType.DMA((2,))],
        compiler_params=room(56),
        name="normed_rows",
    )(place, first, second, residual, before, gain, flags)


def down_kernel(place, near, far, *refs):
    *pieces, keep, send, ws, sems = refs
    sp, tp = place[0], place[1]
    low, high, core = (sp // 2) % 2, sp // 4, tp % 2
    width = pieces[0].shape[1]
    copies = []
    for k, piece in enumerate(pieces):
        slot = 2 * (low ^ (k % 2) ^ core) + (high ^ (k // 2))
        dst = ws.at[:, pl.ds(pl.multiple_of(slot * width, width), width)]
        copies.append(pltpu.make_async_copy(piece, dst, sems.at[k]))
        copies[-1].start()
    for copy in copies:
        copy.wait()
    for out, base in ((send, 2 * width), (keep, 0)):
        for m, hidden in enumerate((near, far)):
            term = jnp.dot(
                hidden[...], ws[:, base : base + 2 * width], preferred_element_type=jnp.float32
            )
            for owner_x in range(2):
                out[owner_x, m] = term[:, owner_x * width : (owner_x + 1) * width].astype(out.dtype)


def down_terms(place, near, far, pieces):
    shape = (2, 2, near.shape[0], pieces[0].shape[1])
    shape = jax.ShapeDtypeStruct(shape, jnp.bfloat16)
    anywhere = pl.BlockSpec(memory_space=pl.ANY)
    return pl.pallas_call(
        down_kernel,
        in_specs=[pl.BlockSpec(memory_space=pltpu.SMEM), vmem(), vmem()] + [anywhere] * len(pieces),
        out_specs=[vmem(), vmem()],
        out_shape=[shape, shape],
        scratch_shapes=[
            pltpu.VMEM((pieces[0].shape[0], len(pieces) * pieces[0].shape[1]), jnp.bfloat16),
            pltpu.SemaphoreType.DMA((len(pieces),)),
        ],
        compiler_params=room(12),
        name="down_terms",
    )(place, near, far, *pieces)


def reduced(keep, send, x, x_first):
    rows, cols = keep.shape[2:]
    own = jnp.zeros((1,), jnp.int32)
    came = swapped(send, tp_mask=1)
    keep, send = merge(x if x_first else own, keep, came, 0 if x_first else 1)
    came = swapped(send, *((0, 2) if x_first else (2, 0)))
    parts = lambda array: array.reshape(2, 2, rows // 2, cols)
    keep, send = merge(own if x_first else x, parts(keep), parts(came), 0)
    came = swapped(send, *((2, 0) if x_first else (0, 2)))
    return keep.reshape(rows, cols), came.reshape(rows, cols)


def local_heads(came, query_rows, key_rows, value_rows, doc_ids, sink_logit):
    rows = query_rows.shape[0]
    kv_local = key_rows.shape[1] // HD
    heads_local = query_rows.shape[1] // HD
    groups = heads_local // kv_local
    reach = WIN + TAIL
    offset = lax.axis_index("sp") * rows
    at = 4 * HD * WIN // LANES
    wide = lambda lines: jnp.concatenate(
        [lines[i : i + TAIL] for i in range(0, lines.shape[0], TAIL)], axis=1
    )
    q_lines = TAIL * query_rows.shape[1] // LANES
    prev_keys, prev_values = (
        jnp.concatenate([came[i : i + HD], came[i + HD : i + 2 * HD]], axis=1)[:, 2 * WIN - reach :]
        for i in (0, 2 * HD)
    )
    prev_docs = came[at : at + 2].reshape(2 * LANES)[2 * LANES - reach :].astype(jnp.int32)
    at = at + TAIL
    prev_queries = wide(came[at : at + q_lines])
    prev_residual = wide(came[at + q_lines :])
    all_keys = jnp.concatenate([prev_keys, key_rows.T], axis=1).T.reshape(rows + reach, kv_local, HD)
    all_values = jnp.concatenate([prev_values, value_rows.T], axis=1).T
    all_values = all_values.reshape(rows + reach, kv_local, HD)
    all_docs = jnp.concatenate([prev_docs, doc_ids])
    key_pos = offset - reach + jnp.arange(rows + reach, dtype=jnp.int32)
    query_pos = offset - TAIL + jnp.arange(rows + TAIL, dtype=jnp.int32)
    queries = jnp.concatenate([prev_queries, query_rows]).reshape(rows + TAIL, kv_local, groups, HD)
    sink = sink_logit.reshape(kv_local, groups, 1, 1)
    pieces = attend(
        queries, all_keys, all_values, query_pos, key_pos, all_docs[WIN:], all_docs, sink
    )
    return pieces.reshape(rows + TAIL, heads_local * HD), prev_docs, prev_residual


def paired(
    query_rows,
    key_rows,
    value_rows,
    doc_ids,
    sink_logit,
    residual,
    out_proj,
    mix_gain,
    gate_proj,
    value_proj,
    gate_taps,
    value_taps,
    down_proj,
    final_gain,
):
    rows, width = residual.shape
    n_tp = lax.axis_size("tp")
    quarter = rows // n_tp
    share = width // n_tp
    sp, tp = lax.axis_index("sp"), lax.axis_index("tp")
    y, low = sp % 2, (sp // 2) % 2
    x, core = tp // 2, tp % 2
    place = jnp.stack([sp, tp]).astype(jnp.int32)
    one = lambda index: index.astype(jnp.int32)[None]
    low_at, x_at, core_at = one(low), one(x), one(core)

    docs_rows = doc_ids[rows - 2 * LANES :].astype(jnp.bfloat16).reshape(2, LANES)
    docs_rows = jnp.pad(docs_rows, ((0, TAIL - 2), (0, 0)))
    own, other, halo = prepared(
        low_at, gate_proj, value_proj, query_rows, key_rows, value_rows, docs_rows, residual
    )
    came_halo = passed_along(halo, "sp", 1)
    from_z = [own, swapped(other, 2), swapped(own, 4), swapped(other, 6)]
    up_weights = []
    for piece in from_z:
        up_weights += [piece, swapped(piece, 1)]
    own, other = row_halves(low_at, down_proj)
    down_same = [own, swapped(other, 2), swapped(own, 4), swapped(other, 6)]
    down_far = [swapped(piece, 1) for piece in down_same]

    heads, prev_docs, prev_residual = local_heads(
        came_halo, query_rows, key_rows, value_rows, doc_ids, sink_logit
    )
    docs = jnp.concatenate([prev_docs[-2:], doc_ids])
    flags = jnp.stack([docs[1:-1] == doc_ids, docs[:-2] == doc_ids]).astype(jnp.float32)
    flags = lax.dynamic_slice_in_dim(flags, tp * quarter, quarter, 1)
    flags = jnp.pad(flags, ((0, TAIL - 2), (0, 0)))
    keep, send = project(place, heads, out_proj, quarter)
    came = swapped(send, tp_mask=1)
    keep, send = merge(x_at, keep[:, None], came[:, None], 0, 56)
    came = swapped(send, tp_mask=2)
    normed = normed_rows(
        place, keep[0], came[0], residual, prev_residual, mix_gain[None, :], flags
    )
    near = [normed, swapped(normed, tp_mask=2)]
    near += [swapped(near[0], tp_mask=1), swapped(near[1], tp_mask=1)]
    normed = swapped(normed, sp_mask=2)
    far = [normed, swapped(normed, tp_mask=2)]
    far += [swapped(far[0], tp_mask=1), swapped(far[1], tp_mask=1)]

    cols = gate_proj.shape[1]
    half = cols // 2
    main = half // LANES * LANES
    rest = half - main
    cut = lambda taps, start, size: lax.dynamic_slice_in_dim(taps, start, size, 1)
    mains = [cut(t, low * (cols - main), main) for t in (gate_taps, value_taps)]
    rests = [cut(t, main + low * rest, rest) for t in (gate_taps, value_taps)]
    mains = jnp.stack([t.reshape(TAPS, main // LANES, LANES) for t in mains], axis=2)
    taps = jnp.concatenate([mains.reshape(TAPS, 2 * main), *rests], axis=1)
    taps = jnp.pad(taps, ((0, 8 - TAPS), (0, 0)))

    near, own_normed = up_hidden(place, near, up_weights, taps, share)
    far, _ = up_hidden(place, far, up_weights, taps, share)
    terms = down_terms(place, near, far, down_same)
    ffn_same = reduced(*terms, x_at, False)
    terms = down_terms(place, near, far, down_far)
    ffn_far = reduced(*terms, x_at, True)
    add = lambda pair: pair[0].astype(jnp.float32) + pair[1].astype(jnp.float32)
    ffn_same, ffn_far = add(ffn_same), add(ffn_far)
    ffn_own = jnp.where(
        y == 0,
        jnp.concatenate([ffn_same, ffn_far], axis=1),
        jnp.concatenate([ffn_far, ffn_same], axis=1),
    )
    second_sum = mix_scale * own_normed.astype(jnp.float32) + ffn_own
    row_sum, row_squares = lax.psum(
        (jnp.sum(second_sum, axis=1), jnp.sum(second_sum * second_sum, axis=1)), "tp"
    )
    mean = row_sum / width
    var = row_squares / width - mean * mean
    return (
        (second_sum - mean[:, None]) * lax.rsqrt(var + norm_eps)[:, None] * final_gain[None, :]
    ).astype(jnp.bfloat16)


def on_device(
    query_rows,
    key_rows,
    value_rows,
    doc_ids,
    sink_logit,
    residual,
    out_proj,
    mix_gain,
    gate_proj,
    value_proj,
    gate_taps,
    value_taps,
    down_proj,
    final_gain,
):
    rows = query_rows.shape[0]
    kv_local = key_rows.shape[1] // HD
    heads_local = query_rows.shape[1] // HD
    groups = heads_local // kv_local
    offset = lax.axis_index("sp") * rows
    prev_keys, prev_values, prev_docs = passed_along(
        (key_rows[rows - WIN :], value_rows[rows - WIN :], doc_ids[rows - WIN :]), "sp", 1
    )
    all_keys = jnp.concatenate([prev_keys, key_rows]).reshape(rows + WIN, kv_local, HD)
    all_values = jnp.concatenate([prev_values, value_rows]).reshape(rows + WIN, kv_local, HD)
    all_docs = jnp.concatenate([prev_docs, doc_ids])
    key_pos = offset - WIN + jnp.arange(rows + WIN, dtype=jnp.int32)
    query_pos = offset + jnp.arange(rows, dtype=jnp.int32)
    queries = query_rows.reshape(rows, kv_local, groups, HD)
    sink = sink_logit.reshape(kv_local, groups, 1, 1)
    pieces = attend(queries, all_keys, all_values, query_pos, key_pos, doc_ids, all_docs, sink)
    heads = pieces.reshape(rows, heads_local * HD)
    partial_value = jnp.dot(heads, out_proj, preferred_element_type=jnp.float32)
    width = residual.shape[1]
    share = width // lax.axis_size("tp")
    col_start = lax.axis_index("tp") * share
    attn_total = lax.psum(partial_value.astype(jnp.bfloat16), "tp").astype(jnp.float32)
    first_sum = mix_scale * residual.astype(jnp.float32) + attn_total
    mean = jnp.mean(first_sum, axis=1, keepdims=True)
    var = jnp.mean(jnp.square(first_sum - mean), axis=1, keepdims=True)
    normed = ((first_sum - mean) * lax.rsqrt(var + norm_eps) * mix_gain[None, :]).astype(
        jnp.bfloat16
    )
    normed_own = lax.dynamic_slice_in_dim(normed, col_start, share, 1)
    up_gate = jnp.dot(
        normed,
        lax.all_gather(gate_proj, "sp", axis=0, tiled=True),
        preferred_element_type=jnp.float32,
    )
    up_value = jnp.dot(
        normed,
        lax.all_gather(value_proj, "sp", axis=0, tiled=True),
        preferred_element_type=jnp.float32,
    )
    up_gate = up_gate.astype(jnp.bfloat16)
    up_value = up_value.astype(jnp.bfloat16)
    lag_rows = TAPS - 1
    prev_gate, prev_value = passed_along(
        (up_gate[rows - lag_rows :], up_value[rows - lag_rows :]), "sp", 1
    )
    tail_docs = prev_docs[WIN - lag_rows :]
    conv_gate = depthwise(prev_gate, up_gate, gate_taps, tail_docs, doc_ids)
    conv_value = depthwise(prev_value, up_value, value_taps, tail_docs, doc_ids)
    hidden = (jax.nn.gelu(conv_gate) * conv_value).astype(jnp.bfloat16)
    terms = jnp.dot(
        hidden,
        lax.all_gather(down_proj, "sp", axis=1, tiled=True),
        preferred_element_type=jnp.float32,
    )
    ffn_own = lax.psum_scatter(
        terms.astype(jnp.bfloat16), "tp", scatter_dimension=1, tiled=True
    ).astype(jnp.float32)
    second_sum = mix_scale * normed_own.astype(jnp.float32) + ffn_own
    row_sum, row_squares = lax.psum(
        (jnp.sum(second_sum, axis=1), jnp.sum(second_sum * second_sum, axis=1)), "tp"
    )
    mean = row_sum / width
    var = row_squares / width - mean * mean
    return (
        (second_sum - mean[:, None]) * lax.rsqrt(var + norm_eps)[:, None] * final_gain[None, :]
    ).astype(jnp.bfloat16)


def solution(mesh):
    placed = (
        P("sp", "tp"),
        P("sp", "tp"),
        P("sp", "tp"),
        P("sp"),
        P("tp"),
        P("sp", None),
        P("tp", None),
        P(),
        P("sp", "tp"),
        P("sp", "tp"),
        P(None, "tp"),
        P(None, "tp"),
        P("tp", "sp"),
        P("tp"),
    )
    fits = mesh.shape["sp"] == 2 * mesh.shape["tp"] and mesh.shape["tp"] == 4
    return jax.shard_map(
        paired if fits else on_device,
        mesh=mesh,
        in_specs=placed,
        out_specs=P("sp", "tp"),
        check_vma=False,
    )
```

```python
import functools
import math

import jax
import jax.numpy as jnp
from jax import lax
from jax.experimental import pallas as pl
from jax.experimental.pallas import tpu as pltpu
from jax.sharding import PartitionSpec as P


HD = 64
WIN = 128
TAPS = 3
LANES = 128
TAIL = 8
RS_ROOM = 56


mix_scale = math.sqrt(2.0)
norm_eps = 1e-05


def passed_along(block, axis, distance):
    devices = range(lax.axis_size(axis))
    route = [(i - distance, i) for i in devices if i - distance in devices]
    return lax.ppermute(block, axis, route)


def swapped(block, sp_mask=0, tp_mask=0):
    n_sp, n_tp = lax.axis_size("sp"), lax.axis_size("tp")
    if not tp_mask:
        return lax.ppermute(block, "sp", [(i, i ^ sp_mask) for i in range(n_sp)])
    if not sp_mask:
        return lax.ppermute(block, "tp", [(i, i ^ tp_mask) for i in range(n_tp)])
    route = [
        (i * n_tp + j, (i ^ sp_mask) * n_tp + (j ^ tp_mask))
        for i in range(n_sp)
        for j in range(n_tp)
    ]
    return lax.ppermute(block, ("sp", "tp"), route)


def attend(query_block, key_block, value_block, query_pos, key_pos, query_doc, key_doc, sink):
    head_size = query_block.shape[-1]
    scores = jnp.einsum(
        "qkgd,skd->kgqs", query_block, key_block, preferred_element_type=jnp.float32
    ) * head_size ** (-0.5)
    diff = query_pos[:, None] - key_pos[None, :]
    valid = (
        (diff >= 0)
        & (diff < WIN)
        & (query_doc[:, None] == key_doc[None, :])
        & (key_pos[None, :] >= 0)
    )
    scores = jnp.where(valid[None, None], scores, -1e30)
    top = jnp.maximum(jnp.max(scores, axis=-1, keepdims=True), sink)
    weights = jnp.exp(scores - top)
    total = jnp.sum(weights, axis=-1, keepdims=True) + jnp.exp(sink - top)
    probs = (weights / total).astype(jnp.bfloat16)
    out = jnp.einsum("kgqs,skd->qkgd", probs, value_block, preferred_element_type=jnp.float32)
    return out.astype(jnp.bfloat16)


def depthwise(tail, current, taps, tail_docs, docs):
    extended = jnp.concatenate([tail, current])
    ext_docs = jnp.concatenate([tail_docs, docs])
    lag_rows = tail.shape[0]
    count = current.shape[0]
    total = jnp.zeros(current.shape, jnp.float32)
    for lag in range(lag_rows + 1):
        start = lag_rows - lag
        same = (ext_docs[start : start + count] == docs)[:, None]
        rows = extended[start : start + count].astype(jnp.float32)
        total = total + taps[lag][None, :] * jnp.where(same, rows, 0.0)
    return total


def room(mib):
    return pltpu.CompilerParams(vmem_limit_bytes=mib << 20)


def hbm():
    return pl.BlockSpec(memory_space=pltpu.HBM)


def vmem():
    return pl.BlockSpec(memory_space=pltpu.VMEM)


def prepare_kernel(
    which, gates, values_in, queries, keys, values, docs, residual, own, other, halo, *scratch
):
    q, k, v, r, gate, value, sems = scratch
    cols = gate.shape[1]
    rows = queries.shape[0]
    whole = [
        pltpu.make_async_copy(src, dst, sems.at[4 + i])
        for i, (src, dst) in enumerate(((gates, gate), (values_in, value)))
    ]
    for copy in whole:
        copy.start()
    copies = [
        pltpu.make_async_copy(src.at[pl.ds(rows - TAIL, TAIL)], dst, sems.at[i])
        for i, (src, dst) in enumerate(((queries, q), (residual, r)))
    ] + [
        pltpu.make_async_copy(src.at[:, pl.ds(rows - 2 * WIN, 2 * WIN)], dst, sems.at[2 + i])
        for i, (src, dst) in enumerate(((keys, k), (values, v)))
    ]
    for copy in copies:
        copy.start()
    for copy in copies:
        copy.wait()
    at = 0
    last = docs[docs.shape[0] - 2 :, :].astype(jnp.float32)
    last = jnp.concatenate([last, jnp.zeros((TAIL - 2, LANES), jnp.float32)])
    for src in (k, v, last.astype(halo.dtype), q, r):
        for n in range(0, src.shape[1], LANES):
            halo[at : at + src.shape[0], :] = src[:, n : n + LANES]
            at += src.shape[0]
    for copy in whole:
        copy.wait()
    half = cols // 2
    main = half // LANES * LANES
    rest = half - main

    def emit(part, out):
        start = part * (cols - main)
        for n in range(0, main, LANES):
            out[:, 2 * n : 2 * n + LANES] = gate[:, start + n : start + n + LANES]
            out[:, 2 * n + LANES : 2 * n + 2 * LANES] = value[:, start + n : start + n + LANES]
        left = gate[:, main : main + LANES].astype(jnp.float32)
        right = value[:, main : main + LANES].astype(jnp.float32)
        if part:
            left = pltpu.roll(left, rest, 1)
        else:
            right = pltpu.roll(right, rest, 1)
        lane = lax.broadcasted_iota(jnp.int32, left.shape, 1)
        out[:, 2 * main :] = jnp.where(lane < rest, left, right).astype(out.dtype)

    @pl.when(which[0] == 0)
    def _():
        emit(0, own)
        emit(1, other)

    @pl.when(which[0] != 0)
    def _():
        emit(1, own)
        emit(0, other)


def prepared(which, gate, value, queries, keys, values, docs, residual):
    shape = jax.ShapeDtypeStruct(gate.shape, gate.dtype)
    lines = 4 * HD * WIN // LANES + TAIL + TAIL * (queries.shape[1] + residual.shape[1]) // LANES
    scratch = [(TAIL, queries.shape[1]), (HD, 2 * WIN), (HD, 2 * WIN)]
    scratch += [(TAIL, residual.shape[1]), gate.shape, gate.shape]
    return pl.pallas_call(
        prepare_kernel,
        in_specs=[pl.BlockSpec(memory_space=pltpu.SMEM)] + [hbm()] * 5 + [vmem(), hbm()],
        out_specs=[vmem()] * 3,
        out_shape=[shape, shape, jax.ShapeDtypeStruct((lines, LANES), jnp.bfloat16)],
        scratch_shapes=[pltpu.VMEM(size, jnp.bfloat16) for size in scratch]
        + [pltpu.SemaphoreType.DMA((6,))],
        compiler_params=room(56),
        name="prepare",
    )(which, gate, value, queries, keys.T, values.T, docs, residual)


def row_halves_kernel(which, down, own, other, sems):
    rows = down.shape[0]
    half = rows // 2
    main = half // LANES * LANES
    rest = half - main
    for f, out in enumerate((own, other)):
        part = which[0] ^ f
        start = pl.multiple_of(part * (rows - main), 2 * TAIL)
        left = pl.multiple_of(main + part * rest, 2 * TAIL)
        copies = [
            pltpu.make_async_copy(
                down.at[pl.ds(start, main)], out.at[pl.ds(0, main)], sems.at[f, 0]
            ),
            pltpu.make_async_copy(
                down.at[pl.ds(left, rest)], out.at[pl.ds(main, rest)], sems.at[f, 1]
            ),
        ]
        for copy in copies:
            copy.start()
    for f, out in enumerate((own, other)):
        pltpu.make_async_copy(
            down.at[pl.ds(0, main)], out.at[pl.ds(0, main)], sems.at[f, 0]
        ).wait()
        pltpu.make_async_copy(
            down.at[pl.ds(0, rest)], out.at[pl.ds(main, rest)], sems.at[f, 1]
        ).wait()


def row_halves(which, down):
    shape = jax.ShapeDtypeStruct((down.shape[0] // 2, down.shape[1]), down.dtype)
    return pl.pallas_call(
        row_halves_kernel,
        in_specs=[pl.BlockSpec(memory_space=pltpu.SMEM), hbm()],
        out_specs=[vmem(), vmem()],
        out_shape=[shape, shape],
        scratch_shapes=[pltpu.SemaphoreType.DMA((2, 2))],
        compiler_params=room(56),
        name="row_halves",
    )(which, down)


def up_kernel(place, *refs, pieces, quarter):
    chunks = (refs[:4], refs[4:8])
    weights = refs[8 : 8 + pieces]
    taps, *hiddens, own_normed, xs, ws, up, flags, same, sems = refs[8 + pieces :]
    sp, tp = place[0], place[1]
    x, core = tp // 2, tp % 2
    piece_rows = weights[0].shape[0]
    block = 4 * quarter

    def rows_in(m):
        copies = []
        for i, chunk in enumerate(chunks[m]):
            number = (x ^ (i % 2)) * 2 + (core ^ (i // 2))
            parts = (
                (
                    chunk.at[pl.ds(TAIL, quarter)],
                    xs.at[m, pl.ds(pl.multiple_of(TAIL + number * quarter, TAIL), quarter)],
                ),
                (chunk.at[pl.ds(0, TAIL), pl.ds(0, LANES)], flags.at[m, number]),
            )
            for f, (src, dst) in enumerate(parts):
                copies.append(pltpu.make_async_copy(src, dst, sems.at[m, 2 * i + f]))
                copies[-1].start()

            @pl.when(number == 0)
            def _(chunk=chunk):
                pltpu.make_async_copy(
                    chunk.at[pl.ds(0, TAIL)], xs.at[m, pl.ds(0, TAIL)], sems.at[m, 8]
                ).start()

        copies.append(
            pltpu.make_async_copy(
                chunks[m][0].at[pl.ds(0, TAIL)], xs.at[m, pl.ds(0, TAIL)], sems.at[m, 8]
            )
        )
        return copies

    near = rows_in(0)
    loads = []
    for j in range(pieces):
        dst = ws.at[pl.ds(pl.multiple_of((sp ^ j) * piece_rows, piece_rows), piece_rows)]
        loads.append(pltpu.make_async_copy(weights[j], dst, sems.at[2, j]))
        loads[-1].start()
    far = rows_in(1)
    half = ws.shape[1] // 2
    main = half // LANES * LANES
    rest = half - main
    pair = 2 * LANES
    sub = 64
    line = lax.broadcasted_iota(jnp.int32, (quarter, quarter), 0)
    diagonal = line == lax.broadcasted_iota(jnp.int32, (quarter, quarter), 1)
    ones = jnp.ones((quarter, LANES), jnp.bfloat16)

    def spread_flags(m):
        for i in range(4):
            rows = flags[m, i].astype(jnp.float32)
            for lag in range(2):
                spread = jnp.where(diagonal, rows[lag : lag + 1], 0.0).astype(jnp.bfloat16)
                same[lag, i * quarter : (i + 1) * quarter] = jnp.dot(
                    spread, ones, preferred_element_type=jnp.float32
                )

    def conv(rows, start, tap, one, two):
        lag1 = rows[TAIL - 1 : TAIL - 1 + sub, start : start + LANES]
        lag2 = rows[TAIL - 2 : TAIL - 2 + sub, start : start + LANES]
        return (
            tap[0:1] * rows[TAIL:, start : start + LANES]
            + tap[1:2] * jnp.where(one > 0, lag1, 0.0)
            + tap[2:3] * jnp.where(two > 0, lag2, 0.0)
        )

    def gelu(v):
        inner = v * (math.sqrt(2.0 / math.pi) + (0.044715 * math.sqrt(2.0 / math.pi)) * (v * v))
        return (0.5 * v) * (1.0 + jnp.tanh(inner))

    def mix(hidden):
        def step(i, _):
            at = pl.ds(pl.multiple_of(i * sub, sub), sub)
            reach = pl.ds(pl.multiple_of(i * sub, sub), sub + TAIL)
            one, two = same[0, at, :], same[1, at, :]
            for n in range(0, main, LANES):
                rows = up[reach, 2 * n : 2 * n + pair]
                tap = taps[:, 2 * n : 2 * n + pair]
                h = gelu(conv(rows, 0, tap[:, :LANES], one, two))
                h = h * conv(rows, LANES, tap[:, LANES:], one, two)
                hidden[at, n : n + LANES] = h.astype(hidden.dtype)
            mixed = conv(up[reach, 2 * main :], 0, taps[:, 2 * main :], one, two)
            h = gelu(mixed) * pltpu.roll(mixed, rest, 1)
            hidden[at, main:] = h[:, :rest].astype(hidden.dtype)
            return 0

        lax.fori_loop(0, block // sub, step, 0)

    depth = ws.shape[0] // 2
    for copy in (*near, *loads[: pieces // 2]):
        copy.wait()
    first = sp // (pieces // 2)
    at = pl.ds(pl.multiple_of(first * depth, depth), depth)
    up[...] = jnp.dot(xs[0, :, at], ws[at, :], preferred_element_type=jnp.float32)
    spread_flags(0)
    for copy in loads[pieces // 2 :]:
        copy.wait()
    at = pl.ds(pl.multiple_of((1 - first) * depth, depth), depth)
    up[...] += jnp.dot(xs[0, :, at], ws[at, :], preferred_element_type=jnp.float32)
    mix(hiddens[0])
    for copy in far:
        copy.wait()
    spread_flags(1)
    up[...] = jnp.dot(xs[1], ws[...], preferred_element_type=jnp.float32)
    mix(hiddens[1])
    share = own_normed.shape[1]
    own_normed[...] = xs[0, TAIL:, pl.ds(pl.multiple_of(tp * share, share), share)]


def up_hidden(place, near, far, weights, taps, share):
    quarter = near[0].shape[0] - TAIL
    width = near[0].shape[1]
    block = 4 * quarter
    cols = weights[0].shape[1]
    anywhere = pl.BlockSpec(memory_space=pl.ANY)
    return pl.pallas_call(
        functools.partial(up_kernel, pieces=len(weights), quarter=quarter),
        in_specs=[pl.BlockSpec(memory_space=pltpu.SMEM)]
        + [anywhere] * (8 + len(weights))
        + [vmem()],
        out_specs=[vmem()] * 3,
        out_shape=[
            jax.ShapeDtypeStruct((block, cols // 2), jnp.bfloat16),
            jax.ShapeDtypeStruct((block, cols // 2), jnp.bfloat16),
            jax.ShapeDtypeStruct((block, share), jnp.bfloat16),
        ],
        scratch_shapes=[
            pltpu.VMEM((2, block + TAIL, width), jnp.bfloat16),
            pltpu.VMEM((width, cols), jnp.bfloat16),
            pltpu.VMEM((block + TAIL, cols), jnp.float32),
            pltpu.VMEM((2, 4, TAIL, LANES), jnp.bfloat16),
            pltpu.VMEM((2, block, LANES), jnp.float32),
            pltpu.SemaphoreType.DMA((3, max(9, len(weights)))),
        ],
        compiler_params=room(24),
        name="up_hidden",
    )(place, *near, *far, *weights, taps)


def project_kernel(place, heads, weights, keep, send, left, right, made, came, went, *, quarter):
    core = place[1] % 2
    count = right.shape[0]
    wide = right.shape[2]
    loads = [pltpu.make_async_copy(heads, left, came.at[count])]
    for n in range(count):
        cols = pl.ds(n * wide, wide)
        loads.append(pltpu.make_async_copy(weights.at[:, cols], right.at[n], came.at[n]))
    for copy in loads:
        copy.start()
    loads[0].wait()
    stores = []
    for n in range(count):
        loads[1 + n].wait()
        term = jnp.dot(left[...], right[n], preferred_element_type=jnp.float32)
        made[n] = term.astype(made.dtype)
        for f, (out, owner) in enumerate(((send, 1 - core), (keep, core))):
            for x in range(2):
                start = pl.multiple_of((2 * x + owner) * quarter, quarter)
                copy = pltpu.make_async_copy(
                    made.at[n, pl.ds(start, quarter + TAIL)],
                    out.at[x, :, pl.ds(n * wide, wide)],
                    went.at[n, 2 * f + x],
                )
                copy.start()
                stores.append(copy)
    for copy in stores:
        copy.wait()


def project(place, heads, weights, quarter):
    count, rows = 4, heads.shape[0]
    depth, width = weights.shape
    shape = jax.ShapeDtypeStruct((2, quarter + TAIL, width), jnp.bfloat16)
    anywhere = pl.BlockSpec(memory_space=pl.ANY)
    return pl.pallas_call(
        functools.partial(project_kernel, quarter=quarter),
        in_specs=[pl.BlockSpec(memory_space=pltpu.SMEM), anywhere, anywhere],
        out_specs=[anywhere, anywhere],
        out_shape=[shape, shape],
        scratch_shapes=[
            pltpu.VMEM((rows, depth), jnp.bfloat16),
            pltpu.VMEM((count, depth, width // count), jnp.bfloat16),
            pltpu.VMEM((count, rows, width // count), jnp.bfloat16),
            pltpu.SemaphoreType.DMA((count + 1,)),
            pltpu.SemaphoreType.DMA((count, 4)),
        ],
        compiler_params=room(RS_ROOM),
        name="project",
    )(place, heads, weights)


def merge_kernel(which, first, second, keep, send):
    own = which[0]
    for out, part in ((send, 1 - own), (keep, own)):
        out[...] = first[part] + second[part]


def merge(which, first, second):
    shape = jax.ShapeDtypeStruct(first.shape[1:], jnp.bfloat16)
    return pl.pallas_call(
        merge_kernel,
        in_specs=[pl.BlockSpec(memory_space=pltpu.SMEM), vmem(), vmem()],
        out_specs=[vmem(), vmem()],
        out_shape=[shape, shape],
        compiler_params=room(RS_ROOM),
        name="merge",
    )(which, first, second)


def fold_kernel(which, first, second, keep_a, send_a, keep_b, send_b):
    own = which[0]
    half = first.shape[3] // 2
    for l in range(2):
        for out, part in ((send_a, 1 - own), (keep_a, own)):
            out[l] = first[part, l, :, :half] + second[part, l, :, :half]
    for x in range(2):
        for out, part in ((send_b, 1), (keep_b, 0)):
            out[x] = first[x, part, :, half:] + second[x, part, :, half:]


def fold(which, first, second):
    _, _, rows, cols = first.shape
    shape = jax.ShapeDtypeStruct((2, rows, cols // 2), jnp.bfloat16)
    return pl.pallas_call(
        fold_kernel,
        in_specs=[pl.BlockSpec(memory_space=pltpu.SMEM), vmem(), vmem()],
        out_specs=[vmem()] * 4,
        out_shape=[shape] * 4,
        compiler_params=room(4),
        name="fold",
    )(which, first, second)


def refold_kernel(which, keep_a, came_a, keep_b, came_b, stay_a, send_a, stay_b, send_b):
    own = which[0]
    stay_a[...] = keep_a[0] + came_a[0]
    send_a[...] = keep_a[1] + came_a[1]
    stay_b[...] = keep_b[own] + came_b[own]
    send_b[...] = keep_b[1 - own] + came_b[1 - own]


def refold(which, *arrays):
    shape = jax.ShapeDtypeStruct(arrays[0].shape[1:], jnp.bfloat16)
    return pl.pallas_call(
        refold_kernel,
        in_specs=[pl.BlockSpec(memory_space=pltpu.SMEM)] + [vmem()] * 4,
        out_specs=[vmem()] * 4,
        out_shape=[shape] * 4,
        compiler_params=room(4),
        name="refold",
    )(which, *arrays)


def norm_kernel(place, first, second, residual, before, gain, flags, out, base, sems):
    tp = place[1]
    rows = first.shape[0]
    quarter = rows - TAIL
    start = pl.multiple_of(tp * quarter, quarter)
    body = pltpu.make_async_copy(
        residual.at[pl.ds(start, quarter)], base.at[pl.ds(TAIL, quarter)], sems.at[0]
    )
    body.start()
    top = base.at[pl.ds(0, TAIL)]

    @pl.when(tp == 0)
    def _():
        pltpu.make_async_copy(before, top, sems.at[1]).start()

    @pl.when(tp != 0)
    def _():
        at = pl.multiple_of(jnp.maximum(start - TAIL, 0), TAIL)
        pltpu.make_async_copy(residual.at[pl.ds(at, TAIL)], top, sems.at[1]).start()

    pltpu.make_async_copy(before, top, sems.at[1]).wait()
    body.wait()
    group = 64
    for r in range(0, rows, group):
        at = slice(r, min(r + group, rows))
        total = first[at].astype(jnp.float32) + second[at].astype(jnp.float32)
        total = mix_scale * base[at].astype(jnp.float32) + total
        mean = jnp.mean(total, axis=1, keepdims=True)
        var = jnp.mean(total * total, axis=1, keepdims=True) - mean * mean
        out[at] = ((total - mean) * lax.rsqrt(var + norm_eps) * gain[...]).astype(out.dtype)
    line = lax.broadcasted_iota(jnp.int32, (TAIL, LANES), 0)
    rows_of = out[:TAIL, :LANES].astype(jnp.float32)
    out[:TAIL, :LANES] = jnp.where(line < 2, flags[...], rows_of).astype(out.dtype)


def normed_rows(place, first, second, residual, before, gain, flags):
    return pl.pallas_call(
        norm_kernel,
        in_specs=[pl.BlockSpec(memory_space=pltpu.SMEM), vmem(), vmem(), hbm(), hbm(), vmem(), vmem()],
        out_specs=vmem(),
        out_shape=jax.ShapeDtypeStruct(first.shape, jnp.bfloat16),
        scratch_shapes=[pltpu.VMEM(first.shape, jnp.bfloat16), pltpu.SemaphoreType.DMA((2,))],
        compiler_params=room(RS_ROOM),
        name="normed_rows",
    )(place, first, second, residual, before, gain, flags)


def down_kernel(place, near, far, *refs):
    *pieces, keep, send, ws, sems = refs
    sp, tp = place[0], place[1]
    low, high, core = (sp // 2) % 2, sp // 4, tp % 2
    width = pieces[0].shape[1]
    copies = []
    for k, piece in enumerate(pieces):
        slot = 2 * (low ^ (k % 2) ^ core) + (high ^ (k // 2))
        dst = ws.at[:, pl.ds(pl.multiple_of(slot * width, width), width)]
        copies.append(pltpu.make_async_copy(piece, dst, sems.at[k]))
        copies[-1].start()
    for copy in copies:
        copy.wait()
    for out, base in ((send, 2 * width), (keep, 0)):
        for m, hidden in enumerate((near, far)):
            term = jnp.dot(
                hidden[...], ws[:, base : base + 2 * width], preferred_element_type=jnp.float32
            )
            for owner_x in range(2):
                out[owner_x, m] = term[:, owner_x * width : (owner_x + 1) * width].astype(out.dtype)


def down_terms(place, near, far, pieces):
    shape = (2, 2, near.shape[0], pieces[0].shape[1])
    shape = jax.ShapeDtypeStruct(shape, jnp.bfloat16)
    anywhere = pl.BlockSpec(memory_space=pl.ANY)
    return pl.pallas_call(
        down_kernel,
        in_specs=[pl.BlockSpec(memory_space=pltpu.SMEM), vmem(), vmem()] + [anywhere] * len(pieces),
        out_specs=[vmem(), vmem()],
        out_shape=[shape, shape],
        scratch_shapes=[
            pltpu.VMEM((pieces[0].shape[0], len(pieces) * pieces[0].shape[1]), jnp.bfloat16),
            pltpu.SemaphoreType.DMA((len(pieces),)),
        ],
        compiler_params=room(12),
        name="down_terms",
    )(place, near, far, *pieces)


def reduced(keep, send, x):
    came = swapped(send, tp_mask=1)
    keep_a, send_a, keep_b, send_b = fold(x, keep, came)
    came_b = swapped(send_b, sp_mask=2)
    came_a = swapped(send_a, tp_mask=2)
    keep_a, send_a, keep_b, send_b = refold(x, keep_a, came_a, keep_b, came_b)
    came_a = swapped(send_a, sp_mask=2)
    came_b = swapped(send_b, tp_mask=2)
    add = lambda one, two: one.astype(jnp.float32) + two.astype(jnp.float32)
    return jnp.concatenate([add(keep_a, came_a), add(keep_b, came_b)], axis=1)


def local_heads(came, query_rows, key_rows, value_rows, doc_ids, sink_logit):
    rows = query_rows.shape[0]
    kv_local = key_rows.shape[1] // HD
    heads_local = query_rows.shape[1] // HD
    groups = heads_local // kv_local
    reach = WIN + TAIL
    offset = lax.axis_index("sp") * rows
    at = 4 * HD * WIN // LANES
    wide = lambda lines: jnp.concatenate(
        [lines[i : i + TAIL] for i in range(0, lines.shape[0], TAIL)], axis=1
    )
    q_lines = TAIL * query_rows.shape[1] // LANES
    prev_keys, prev_values = (
        jnp.concatenate([came[i : i + HD], came[i + HD : i + 2 * HD]], axis=1)[:, 2 * WIN - reach :]
        for i in (0, 2 * HD)
    )
    prev_docs = came[at : at + 2].reshape(2 * LANES)[2 * LANES - reach :].astype(jnp.int32)
    at = at + TAIL
    prev_queries = wide(came[at : at + q_lines])
    prev_residual = wide(came[at + q_lines :])
    all_keys = jnp.concatenate([prev_keys, key_rows.T], axis=1).T.reshape(rows + reach, kv_local, HD)
    all_values = jnp.concatenate([prev_values, value_rows.T], axis=1).T
    all_values = all_values.reshape(rows + reach, kv_local, HD)
    all_docs = jnp.concatenate([prev_docs, doc_ids])
    key_pos = offset - reach + jnp.arange(rows + reach, dtype=jnp.int32)
    query_pos = offset - TAIL + jnp.arange(rows + TAIL, dtype=jnp.int32)
    queries = jnp.concatenate([prev_queries, query_rows]).reshape(rows + TAIL, kv_local, groups, HD)
    sink = sink_logit.reshape(kv_local, groups, 1, 1)
    pieces = attend(
        queries, all_keys, all_values, query_pos, key_pos, all_docs[WIN:], all_docs, sink
    )
    return pieces.reshape(rows + TAIL, heads_local * HD), prev_docs, prev_residual


def paired(
    query_rows,
    key_rows,
    value_rows,
    doc_ids,
    sink_logit,
    residual,
    out_proj,
    mix_gain,
    gate_proj,
    value_proj,
    gate_taps,
    value_taps,
    down_proj,
    final_gain,
):
    rows, width = residual.shape
    n_tp = lax.axis_size("tp")
    quarter = rows // n_tp
    share = width // n_tp
    sp, tp = lax.axis_index("sp"), lax.axis_index("tp")
    y, low = sp % 2, (sp // 2) % 2
    x, core = tp // 2, tp % 2
    place = jnp.stack([sp, tp]).astype(jnp.int32)
    one = lambda index: index.astype(jnp.int32)[None]
    low_at, x_at, core_at = one(low), one(x), one(core)

    docs_rows = doc_ids.reshape(rows // LANES, LANES)
    own, other, halo = prepared(
        low_at, gate_proj, value_proj, query_rows, key_rows, value_rows, docs_rows, residual
    )
    came_halo = passed_along(halo, "sp", 1)
    from_z = [own, swapped(other, 2), swapped(own, 4), swapped(other, 6)]
    up_weights = []
    for piece in from_z:
        up_weights += [piece, swapped(piece, 1)]
    own, other = row_halves(low_at, down_proj)
    down_same = [own, swapped(other, 2), swapped(own, 4), swapped(other, 6)]
    down_far = [swapped(piece, 1) for piece in down_same]

    heads, prev_docs, prev_residual = local_heads(
        came_halo, query_rows, key_rows, value_rows, doc_ids, sink_logit
    )
    docs = jnp.concatenate([prev_docs[-2:], doc_ids])
    flags = jnp.stack([docs[1:-1] == doc_ids, docs[:-2] == doc_ids]).astype(jnp.float32)
    flags = lax.dynamic_slice_in_dim(flags, tp * quarter, quarter, 1)
    flags = jnp.pad(flags, ((0, TAIL - 2), (0, 0)))
    keep, send = project(place, heads, out_proj, quarter)
    came = swapped(send, tp_mask=1)
    keep, send = merge(x_at, keep, came)
    came = swapped(send, tp_mask=2)
    normed = normed_rows(
        place, keep, came, residual, prev_residual, mix_gain[None, :], flags
    )
    near = [normed, swapped(normed, tp_mask=2)]
    near += [swapped(near[0], tp_mask=1), swapped(near[1], tp_mask=1)]
    normed = swapped(normed, sp_mask=2)
    far = [normed, swapped(normed, tp_mask=2)]
    far += [swapped(far[0], tp_mask=1), swapped(far[1], tp_mask=1)]

    cols = gate_proj.shape[1]
    half = cols // 2
    main = half // LANES * LANES
    rest = half - main
    cut = lambda taps, start, size: lax.dynamic_slice_in_dim(taps, start, size, 1)
    mains = [cut(t, low * (cols - main), main) for t in (gate_taps, value_taps)]
    rests = [cut(t, main + low * rest, rest) for t in (gate_taps, value_taps)]
    mains = jnp.stack([t.reshape(TAPS, main // LANES, LANES) for t in mains], axis=2)
    taps = jnp.concatenate([mains.reshape(TAPS, 2 * main), *rests], axis=1)
    taps = jnp.pad(taps, ((0, 8 - TAPS), (0, 0)))

    near, far, own_normed = up_hidden(place, near, far, up_weights, taps, share)
    terms = down_terms(place, near, far, down_same)
    ffn_same = reduced(*terms, x_at)
    terms = down_terms(place, near, far, down_far)
    ffn_far = reduced(*terms, x_at)
    ffn_own = jnp.where(
        y == 0,
        jnp.concatenate([ffn_same, ffn_far], axis=1),
        jnp.concatenate([ffn_far, ffn_same], axis=1),
    )
    second_sum = mix_scale * own_normed.astype(jnp.float32) + ffn_own
    row_sum, row_squares = lax.psum(
        (jnp.sum(second_sum, axis=1), jnp.sum(second_sum * second_sum, axis=1)), "tp"
    )
    mean = row_sum / width
    var = row_squares / width - mean * mean
    return (
        (second_sum - mean[:, None]) * lax.rsqrt(var + norm_eps)[:, None] * final_gain[None, :]
    ).astype(jnp.bfloat16)


def on_device(
    query_rows,
    key_rows,
    value_rows,
    doc_ids,
    sink_logit,
    residual,
    out_proj,
    mix_gain,
    gate_proj,
    value_proj,
    gate_taps,
    value_taps,
    down_proj,
    final_gain,
):
    rows = query_rows.shape[0]
    kv_local = key_rows.shape[1] // HD
    heads_local = query_rows.shape[1] // HD
    groups = heads_local // kv_local
    offset = lax.axis_index("sp") * rows
    prev_keys, prev_values, prev_docs = passed_along(
        (key_rows[rows - WIN :], value_rows[rows - WIN :], doc_ids[rows - WIN :]), "sp", 1
    )
    all_keys = jnp.concatenate([prev_keys, key_rows]).reshape(rows + WIN, kv_local, HD)
    all_values = jnp.concatenate([prev_values, value_rows]).reshape(rows + WIN, kv_local, HD)
    all_docs = jnp.concatenate([prev_docs, doc_ids])
    key_pos = offset - WIN + jnp.arange(rows + WIN, dtype=jnp.int32)
    query_pos = offset + jnp.arange(rows, dtype=jnp.int32)
    queries = query_rows.reshape(rows, kv_local, groups, HD)
    sink = sink_logit.reshape(kv_local, groups, 1, 1)
    pieces = attend(queries, all_keys, all_values, query_pos, key_pos, doc_ids, all_docs, sink)
    heads = pieces.reshape(rows, heads_local * HD)
    partial_value = jnp.dot(heads, out_proj, preferred_element_type=jnp.float32)
    width = residual.shape[1]
    share = width // lax.axis_size("tp")
    col_start = lax.axis_index("tp") * share
    attn_total = lax.psum(partial_value.astype(jnp.bfloat16), "tp").astype(jnp.float32)
    first_sum = mix_scale * residual.astype(jnp.float32) + attn_total
    mean = jnp.mean(first_sum, axis=1, keepdims=True)
    var = jnp.mean(jnp.square(first_sum - mean), axis=1, keepdims=True)
    normed = ((first_sum - mean) * lax.rsqrt(var + norm_eps) * mix_gain[None, :]).astype(
        jnp.bfloat16
    )
    normed_own = lax.dynamic_slice_in_dim(normed, col_start, share, 1)
    up_gate = jnp.dot(
        normed,
        lax.all_gather(gate_proj, "sp", axis=0, tiled=True),
        preferred_element_type=jnp.float32,
    )
    up_value = jnp.dot(
        normed,
        lax.all_gather(value_proj, "sp", axis=0, tiled=True),
        preferred_element_type=jnp.float32,
    )
    up_gate = up_gate.astype(jnp.bfloat16)
    up_value = up_value.astype(jnp.bfloat16)
    lag_rows = TAPS - 1
    prev_gate, prev_value = passed_along(
        (up_gate[rows - lag_rows :], up_value[rows - lag_rows :]), "sp", 1
    )
    tail_docs = prev_docs[WIN - lag_rows :]
    conv_gate = depthwise(prev_gate, up_gate, gate_taps, tail_docs, doc_ids)
    conv_value = depthwise(prev_value, up_value, value_taps, tail_docs, doc_ids)
    hidden = (jax.nn.gelu(conv_gate) * conv_value).astype(jnp.bfloat16)
    terms = jnp.dot(
        hidden,
        lax.all_gather(down_proj, "sp", axis=1, tiled=True),
        preferred_element_type=jnp.float32,
    )
    ffn_own = lax.psum_scatter(
        terms.astype(jnp.bfloat16), "tp", scatter_dimension=1, tiled=True
    ).astype(jnp.float32)
    second_sum = mix_scale * normed_own.astype(jnp.float32) + ffn_own
    row_sum, row_squares = lax.psum(
        (jnp.sum(second_sum, axis=1), jnp.sum(second_sum * second_sum, axis=1)), "tp"
    )
    mean = row_sum / width
    var = row_squares / width - mean * mean
    return (
        (second_sum - mean[:, None]) * lax.rsqrt(var + norm_eps)[:, None] * final_gain[None, :]
    ).astype(jnp.bfloat16)


def solution(mesh):
    placed = (
        P("sp", "tp"),
        P("sp", "tp"),
        P("sp", "tp"),
        P("sp"),
        P("tp"),
        P("sp", None),
        P("tp", None),
        P(),
        P("sp", "tp"),
        P("sp", "tp"),
        P(None, "tp"),
        P(None, "tp"),
        P("tp", "sp"),
        P("tp"),
    )
    fits = mesh.shape["sp"] == 2 * mesh.shape["tp"] and mesh.shape["tp"] == 4
    return jax.shard_map(
        paired if fits else on_device,
        mesh=mesh,
        in_specs=placed,
        out_specs=P("sp", "tp"),
        check_vma=False,
    )
```

```python
import functools
import math

import jax
import jax.numpy as jnp
from jax import lax
from jax.experimental import pallas as pl
from jax.experimental.pallas import tpu as pltpu
from jax.sharding import PartitionSpec as P


HD = 64
WIN = 128
TAPS = 3
LANES = 128
TAIL = 8
RS_ROOM = 56


mix_scale = math.sqrt(2.0)
norm_eps = 1e-05


def passed_along(block, axis, distance):
    devices = range(lax.axis_size(axis))
    route = [(i - distance, i) for i in devices if i - distance in devices]
    return lax.ppermute(block, axis, route)


def swapped(block, sp_mask=0, tp_mask=0):
    n_sp, n_tp = lax.axis_size("sp"), lax.axis_size("tp")
    if not tp_mask:
        return lax.ppermute(block, "sp", [(i, i ^ sp_mask) for i in range(n_sp)])
    if not sp_mask:
        return lax.ppermute(block, "tp", [(i, i ^ tp_mask) for i in range(n_tp)])
    route = [
        (i * n_tp + j, (i ^ sp_mask) * n_tp + (j ^ tp_mask))
        for i in range(n_sp)
        for j in range(n_tp)
    ]
    return lax.ppermute(block, ("sp", "tp"), route)


def attend(query_block, key_block, value_block, query_pos, key_pos, query_doc, key_doc, sink):
    head_size = query_block.shape[-1]
    scores = jnp.einsum(
        "qkgd,skd->kgqs", query_block, key_block, preferred_element_type=jnp.float32
    ) * head_size ** (-0.5)
    diff = query_pos[:, None] - key_pos[None, :]
    valid = (
        (diff >= 0)
        & (diff < WIN)
        & (query_doc[:, None] == key_doc[None, :])
        & (key_pos[None, :] >= 0)
    )
    scores = jnp.where(valid[None, None], scores, -1e30)
    top = jnp.maximum(jnp.max(scores, axis=-1, keepdims=True), sink)
    weights = jnp.exp(scores - top)
    total = jnp.sum(weights, axis=-1, keepdims=True) + jnp.exp(sink - top)
    probs = (weights / total).astype(jnp.bfloat16)
    out = jnp.einsum("kgqs,skd->qkgd", probs, value_block, preferred_element_type=jnp.float32)
    return out.astype(jnp.bfloat16)


def depthwise(tail, current, taps, tail_docs, docs):
    extended = jnp.concatenate([tail, current])
    ext_docs = jnp.concatenate([tail_docs, docs])
    lag_rows = tail.shape[0]
    count = current.shape[0]
    total = jnp.zeros(current.shape, jnp.float32)
    for lag in range(lag_rows + 1):
        start = lag_rows - lag
        same = (ext_docs[start : start + count] == docs)[:, None]
        rows = extended[start : start + count].astype(jnp.float32)
        total = total + taps[lag][None, :] * jnp.where(same, rows, 0.0)
    return total


def room(mib):
    return pltpu.CompilerParams(vmem_limit_bytes=mib << 20)


def hbm():
    return pl.BlockSpec(memory_space=pltpu.HBM)


def vmem():
    return pl.BlockSpec(memory_space=pltpu.VMEM)


def pack_kernel(queries, keys, values, docs, residual, halo, q, k, v, r, sems):
    rows = queries.shape[0]
    copies = [
        pltpu.make_async_copy(src.at[pl.ds(rows - TAIL, TAIL)], dst, sems.at[i])
        for i, (src, dst) in enumerate(((queries, q), (residual, r)))
    ] + [
        pltpu.make_async_copy(src.at[:, pl.ds(rows - 2 * WIN, 2 * WIN)], dst, sems.at[2 + i])
        for i, (src, dst) in enumerate(((keys, k), (values, v)))
    ]
    for copy in copies:
        copy.start()
    for copy in copies:
        copy.wait()
    at = 0
    last = docs[docs.shape[0] - 2 :, :].astype(jnp.float32)
    last = jnp.concatenate([last, jnp.zeros((TAIL - 2, LANES), jnp.float32)])
    for src in (k, v, last.astype(halo.dtype), q, r):
        for n in range(0, src.shape[1], LANES):
            halo[at : at + src.shape[0], :] = src[:, n : n + LANES]
            at += src.shape[0]


def packed(queries, keys, values, docs, residual):
    lines = 4 * HD * WIN // LANES + TAIL + TAIL * (queries.shape[1] + residual.shape[1]) // LANES
    scratch = [(TAIL, queries.shape[1]), (HD, 2 * WIN), (HD, 2 * WIN), (TAIL, residual.shape[1])]
    return pl.pallas_call(
        pack_kernel,
        in_specs=[hbm(), hbm(), hbm(), vmem(), hbm()],
        out_specs=vmem(),
        out_shape=jax.ShapeDtypeStruct((lines, LANES), jnp.bfloat16),
        scratch_shapes=[pltpu.VMEM(size, jnp.bfloat16) for size in scratch]
        + [pltpu.SemaphoreType.DMA((4,))],
        compiler_params=room(56),
        name="pack",
    )(queries, keys.T, values.T, docs, residual)


def prepare_kernel(which, gates, values, own, other, gate, value, sems):
    cols = gate.shape[1]
    copies = [
        pltpu.make_async_copy(src, dst, sems.at[i])
        for i, (src, dst) in enumerate(((gates, gate), (values, value)))
    ]
    for copy in copies:
        copy.start()
    for copy in copies:
        copy.wait()
    half = cols // 2
    main = half // LANES * LANES
    rest = half - main

    def emit(part, out):
        start = part * (cols - main)
        for n in range(0, main, LANES):
            out[:, 2 * n : 2 * n + LANES] = gate[:, start + n : start + n + LANES]
            out[:, 2 * n + LANES : 2 * n + 2 * LANES] = value[:, start + n : start + n + LANES]
        left = gate[:, main : main + LANES].astype(jnp.float32)
        right = value[:, main : main + LANES].astype(jnp.float32)
        if part:
            left = pltpu.roll(left, rest, 1)
        else:
            right = pltpu.roll(right, rest, 1)
        lane = lax.broadcasted_iota(jnp.int32, left.shape, 1)
        out[:, 2 * main :] = jnp.where(lane < rest, left, right).astype(out.dtype)

    @pl.when(which[0] == 0)
    def _():
        emit(0, own)
        emit(1, other)

    @pl.when(which[0] != 0)
    def _():
        emit(1, own)
        emit(0, other)


def prepared(which, gate, value):
    shape = jax.ShapeDtypeStruct(gate.shape, gate.dtype)
    return pl.pallas_call(
        prepare_kernel,
        in_specs=[pl.BlockSpec(memory_space=pltpu.SMEM), hbm(), hbm()],
        out_specs=[vmem()] * 2,
        out_shape=[shape, shape],
        scratch_shapes=[pltpu.VMEM(gate.shape, gate.dtype)] * 2 + [pltpu.SemaphoreType.DMA((2,))],
        compiler_params=room(56),
        name="prepare",
    )(which, gate, value)


def row_halves_kernel(which, down, own, other, sems):
    rows = down.shape[0]
    half = rows // 2
    main = half // LANES * LANES
    rest = half - main
    for f, out in enumerate((own, other)):
        part = which[0] ^ f
        start = pl.multiple_of(part * (rows - main), 2 * TAIL)
        left = pl.multiple_of(main + part * rest, 2 * TAIL)
        copies = [
            pltpu.make_async_copy(
                down.at[pl.ds(start, main)], out.at[pl.ds(0, main)], sems.at[f, 0]
            ),
            pltpu.make_async_copy(
                down.at[pl.ds(left, rest)], out.at[pl.ds(main, rest)], sems.at[f, 1]
            ),
        ]
        for copy in copies:
            copy.start()
    for f, out in enumerate((own, other)):
        pltpu.make_async_copy(
            down.at[pl.ds(0, main)], out.at[pl.ds(0, main)], sems.at[f, 0]
        ).wait()
        pltpu.make_async_copy(
            down.at[pl.ds(0, rest)], out.at[pl.ds(main, rest)], sems.at[f, 1]
        ).wait()


def row_halves(which, down):
    shape = jax.ShapeDtypeStruct((down.shape[0] // 2, down.shape[1]), down.dtype)
    return pl.pallas_call(
        row_halves_kernel,
        in_specs=[pl.BlockSpec(memory_space=pltpu.SMEM), hbm()],
        out_specs=[vmem(), vmem()],
        out_shape=[shape, shape],
        scratch_shapes=[pltpu.SemaphoreType.DMA((2, 2))],
        compiler_params=room(56),
        name="row_halves",
    )(which, down)


def up_kernel(place, *refs, pieces, quarter):
    chunks = (refs[:4], refs[4:8])
    weights = refs[8 : 8 + pieces]
    taps, *hiddens, own_normed, xs, ws, up, flags, same, sems = refs[8 + pieces :]
    sp, tp = place[0], place[1]
    x, core = tp // 2, tp % 2
    piece_rows = weights[0].shape[0]
    block = 4 * quarter

    def rows_in(m):
        copies = []
        for i, chunk in enumerate(chunks[m]):
            number = (x ^ (i % 2)) * 2 + (core ^ (i // 2))
            parts = (
                (
                    chunk.at[pl.ds(TAIL, quarter)],
                    xs.at[m, pl.ds(pl.multiple_of(TAIL + number * quarter, TAIL), quarter)],
                ),
                (chunk.at[pl.ds(0, TAIL), pl.ds(0, LANES)], flags.at[m, number]),
            )
            for f, (src, dst) in enumerate(parts):
                copies.append(pltpu.make_async_copy(src, dst, sems.at[m, 2 * i + f]))
                copies[-1].start()

            @pl.when(number == 0)
            def _(chunk=chunk):
                pltpu.make_async_copy(
                    chunk.at[pl.ds(0, TAIL)], xs.at[m, pl.ds(0, TAIL)], sems.at[m, 8]
                ).start()

        copies.append(
            pltpu.make_async_copy(
                chunks[m][0].at[pl.ds(0, TAIL)], xs.at[m, pl.ds(0, TAIL)], sems.at[m, 8]
            )
        )
        return copies

    near = rows_in(0)
    loads = []
    for j in range(pieces):
        dst = ws.at[pl.ds(pl.multiple_of((sp ^ j) * piece_rows, piece_rows), piece_rows)]
        loads.append(pltpu.make_async_copy(weights[j], dst, sems.at[2, j]))
        loads[-1].start()
    far = rows_in(1)
    half = ws.shape[1] // 2
    main = half // LANES * LANES
    rest = half - main
    pair = 2 * LANES
    sub = 64
    line = lax.broadcasted_iota(jnp.int32, (quarter, quarter), 0)
    diagonal = line == lax.broadcasted_iota(jnp.int32, (quarter, quarter), 1)
    ones = jnp.ones((quarter, LANES), jnp.bfloat16)

    def spread_flags(m):
        for i in range(4):
            rows = flags[m, i].astype(jnp.float32)
            for lag in range(2):
                spread = jnp.where(diagonal, rows[lag : lag + 1], 0.0).astype(jnp.bfloat16)
                same[lag, i * quarter : (i + 1) * quarter] = jnp.dot(
                    spread, ones, preferred_element_type=jnp.float32
                )

    def conv(rows, start, tap, one, two):
        lag1 = rows[TAIL - 1 : TAIL - 1 + sub, start : start + LANES]
        lag2 = rows[TAIL - 2 : TAIL - 2 + sub, start : start + LANES]
        return (
            tap[0:1] * rows[TAIL:, start : start + LANES]
            + tap[1:2] * jnp.where(one > 0, lag1, 0.0)
            + tap[2:3] * jnp.where(two > 0, lag2, 0.0)
        )

    def gelu(v):
        inner = v * (math.sqrt(2.0 / math.pi) + (0.044715 * math.sqrt(2.0 / math.pi)) * (v * v))
        return (0.5 * v) * (1.0 + jnp.tanh(inner))

    def mix(hidden):
        def step(i, _):
            at = pl.ds(pl.multiple_of(i * sub, sub), sub)
            reach = pl.ds(pl.multiple_of(i * sub, sub), sub + TAIL)
            one, two = same[0, at, :], same[1, at, :]
            for n in range(0, main, LANES):
                rows = up[reach, 2 * n : 2 * n + pair]
                tap = taps[:, 2 * n : 2 * n + pair]
                h = gelu(conv(rows, 0, tap[:, :LANES], one, two))
                h = h * conv(rows, LANES, tap[:, LANES:], one, two)
                hidden[at, n : n + LANES] = h.astype(hidden.dtype)
            mixed = conv(up[reach, 2 * main :], 0, taps[:, 2 * main :], one, two)
            h = gelu(mixed) * pltpu.roll(mixed, rest, 1)
            hidden[at, main:] = h[:, :rest].astype(hidden.dtype)
            return 0

        lax.fori_loop(0, block // sub, step, 0)

    depth = ws.shape[0] // 2
    for copy in (*near, *loads[: pieces // 2]):
        copy.wait()
    first = sp // (pieces // 2)
    at = pl.ds(pl.multiple_of(first * depth, depth), depth)
    up[...] = jnp.dot(xs[0, :, at], ws[at, :], preferred_element_type=jnp.float32)
    spread_flags(0)
    for copy in loads[pieces // 2 :]:
        copy.wait()
    at = pl.ds(pl.multiple_of((1 - first) * depth, depth), depth)
    up[...] += jnp.dot(xs[0, :, at], ws[at, :], preferred_element_type=jnp.float32)
    mix(hiddens[0])
    for copy in far:
        copy.wait()
    spread_flags(1)
    up[...] = jnp.dot(xs[1], ws[...], preferred_element_type=jnp.float32)
    mix(hiddens[1])
    share = own_normed.shape[1]
    own_normed[...] = xs[0, TAIL:, pl.ds(pl.multiple_of(tp * share, share), share)]


def up_hidden(place, near, far, weights, taps, share):
    quarter = near[0].shape[0] - TAIL
    width = near[0].shape[1]
    block = 4 * quarter
    cols = weights[0].shape[1]
    anywhere = pl.BlockSpec(memory_space=pl.ANY)
    return pl.pallas_call(
        functools.partial(up_kernel, pieces=len(weights), quarter=quarter),
        in_specs=[pl.BlockSpec(memory_space=pltpu.SMEM)]
        + [anywhere] * (8 + len(weights))
        + [vmem()],
        out_specs=[vmem()] * 3,
        out_shape=[
            jax.ShapeDtypeStruct((block, cols // 2), jnp.bfloat16),
            jax.ShapeDtypeStruct((block, cols // 2), jnp.bfloat16),
            jax.ShapeDtypeStruct((block, share), jnp.bfloat16),
        ],
        scratch_shapes=[
            pltpu.VMEM((2, block + TAIL, width), jnp.bfloat16),
            pltpu.VMEM((width, cols), jnp.bfloat16),
            pltpu.VMEM((block + TAIL, cols), jnp.float32),
            pltpu.VMEM((2, 4, TAIL, LANES), jnp.bfloat16),
            pltpu.VMEM((2, block, LANES), jnp.float32),
            pltpu.SemaphoreType.DMA((3, max(9, len(weights)))),
        ],
        compiler_params=room(24),
        name="up_hidden",
    )(place, *near, *far, *weights, taps)


def project_kernel(place, heads, weights, keep, send, left, right, made, came, went, *, quarter):
    core = place[1] % 2
    count = right.shape[0]
    wide = right.shape[2]
    loads = [pltpu.make_async_copy(heads, left, came.at[count])]
    for n in range(count):
        cols = pl.ds(n * wide, wide)
        loads.append(pltpu.make_async_copy(weights.at[:, cols], right.at[n], came.at[n]))
    for copy in loads:
        copy.start()
    loads[0].wait()
    stores = []
    for n in range(count):
        loads[1 + n].wait()
        term = jnp.dot(left[...], right[n], preferred_element_type=jnp.float32)
        made[n] = term.astype(made.dtype)
        for f, (out, owner) in enumerate(((send, 1 - core), (keep, core))):
            for x in range(2):
                start = pl.multiple_of((2 * x + owner) * quarter, quarter)
                copy = pltpu.make_async_copy(
                    made.at[n, pl.ds(start, quarter + TAIL)],
                    out.at[x, :, pl.ds(n * wide, wide)],
                    went.at[n, 2 * f + x],
                )
                copy.start()
                stores.append(copy)
    for copy in stores:
        copy.wait()


def project(place, heads, weights, quarter):
    count, rows = 4, heads.shape[0]
    depth, width = weights.shape
    shape = jax.ShapeDtypeStruct((2, quarter + TAIL, width), jnp.bfloat16)
    anywhere = pl.BlockSpec(memory_space=pl.ANY)
    return pl.pallas_call(
        functools.partial(project_kernel, quarter=quarter),
        in_specs=[pl.BlockSpec(memory_space=pltpu.SMEM), anywhere, anywhere],
        out_specs=[anywhere, anywhere],
        out_shape=[shape, shape],
        scratch_shapes=[
            pltpu.VMEM((rows, depth), jnp.bfloat16),
            pltpu.VMEM((count, depth, width // count), jnp.bfloat16),
            pltpu.VMEM((count, rows, width // count), jnp.bfloat16),
            pltpu.SemaphoreType.DMA((count + 1,)),
            pltpu.SemaphoreType.DMA((count, 4)),
        ],
        compiler_params=room(RS_ROOM),
        name="project",
    )(place, heads, weights)


def merge_kernel(which, first, second, keep, send):
    own = which[0]
    for out, part in ((send, 1 - own), (keep, own)):
        out[...] = first[part] + second[part]


def merge(which, first, second):
    shape = jax.ShapeDtypeStruct(first.shape[1:], jnp.bfloat16)
    return pl.pallas_call(
        merge_kernel,
        in_specs=[pl.BlockSpec(memory_space=pltpu.SMEM), vmem(), vmem()],
        out_specs=[vmem(), vmem()],
        out_shape=[shape, shape],
        compiler_params=room(RS_ROOM),
        name="merge",
    )(which, first, second)


def fold_kernel(which, first, second, keep_a, send_a, keep_b, send_b):
    own = which[0]
    half = first.shape[3] // 2
    for l in range(2):
        for out, part in ((send_a, 1 - own), (keep_a, own)):
            out[l] = first[part, l, :, :half] + second[part, l, :, :half]
    for x in range(2):
        for out, part in ((send_b, 1), (keep_b, 0)):
            out[x] = first[x, part, :, half:] + second[x, part, :, half:]


def fold(which, first, second):
    _, _, rows, cols = first.shape
    shape = jax.ShapeDtypeStruct((2, rows, cols // 2), jnp.bfloat16)
    return pl.pallas_call(
        fold_kernel,
        in_specs=[pl.BlockSpec(memory_space=pltpu.SMEM), vmem(), vmem()],
        out_specs=[vmem()] * 4,
        out_shape=[shape] * 4,
        compiler_params=room(4),
        name="fold",
    )(which, first, second)


def refold_kernel(which, keep_a, came_a, keep_b, came_b, stay_a, send_a, stay_b, send_b):
    own = which[0]
    stay_a[...] = keep_a[0] + came_a[0]
    send_a[...] = keep_a[1] + came_a[1]
    stay_b[...] = keep_b[own] + came_b[own]
    send_b[...] = keep_b[1 - own] + came_b[1 - own]


def refold(which, *arrays):
    shape = jax.ShapeDtypeStruct(arrays[0].shape[1:], jnp.bfloat16)
    return pl.pallas_call(
        refold_kernel,
        in_specs=[pl.BlockSpec(memory_space=pltpu.SMEM)] + [vmem()] * 4,
        out_specs=[vmem()] * 4,
        out_shape=[shape] * 4,
        compiler_params=room(4),
        name="refold",
    )(which, *arrays)


def norm_kernel(place, first, second, residual, before, gain, flags, out, base, sems):
    tp = place[1]
    rows = first.shape[0]
    quarter = rows - TAIL
    start = pl.multiple_of(tp * quarter, quarter)
    body = pltpu.make_async_copy(
        residual.at[pl.ds(start, quarter)], base.at[pl.ds(TAIL, quarter)], sems.at[0]
    )
    body.start()
    top = base.at[pl.ds(0, TAIL)]

    @pl.when(tp == 0)
    def _():
        pltpu.make_async_copy(before, top, sems.at[1]).start()

    @pl.when(tp != 0)
    def _():
        at = pl.multiple_of(jnp.maximum(start - TAIL, 0), TAIL)
        pltpu.make_async_copy(residual.at[pl.ds(at, TAIL)], top, sems.at[1]).start()

    pltpu.make_async_copy(before, top, sems.at[1]).wait()
    body.wait()
    group = 64
    for r in range(0, rows, group):
        at = slice(r, min(r + group, rows))
        total = first[at].astype(jnp.float32) + second[at].astype(jnp.float32)
        total = mix_scale * base[at].astype(jnp.float32) + total
        mean = jnp.mean(total, axis=1, keepdims=True)
        var = jnp.mean(total * total, axis=1, keepdims=True) - mean * mean
        out[at] = ((total - mean) * lax.rsqrt(var + norm_eps) * gain[...]).astype(out.dtype)
    line = lax.broadcasted_iota(jnp.int32, (TAIL, LANES), 0)
    rows_of = out[:TAIL, :LANES].astype(jnp.float32)
    out[:TAIL, :LANES] = jnp.where(line < 2, flags[...], rows_of).astype(out.dtype)


def normed_rows(place, first, second, residual, before, gain, flags):
    return pl.pallas_call(
        norm_kernel,
        in_specs=[pl.BlockSpec(memory_space=pltpu.SMEM), vmem(), vmem(), hbm(), hbm(), vmem(), vmem()],
        out_specs=vmem(),
        out_shape=jax.ShapeDtypeStruct(first.shape, jnp.bfloat16),
        scratch_shapes=[pltpu.VMEM(first.shape, jnp.bfloat16), pltpu.SemaphoreType.DMA((2,))],
        compiler_params=room(RS_ROOM),
        name="normed_rows",
    )(place, first, second, residual, before, gain, flags)


def down_kernel(place, near, far, *refs):
    *pieces, keep, send, ws, sems = refs
    if len(pieces) == 3:
        pieces.append(None)
    sp, tp = place[0], place[1]
    low, high, core = (sp // 2) % 2, sp // 4, tp % 2
    width = pieces[0].shape[1]
    copies = []
    for k, piece in enumerate(pieces):
        slot = 2 * (low ^ (k % 2) ^ core) + (high ^ (k // 2))
        dst = ws.at[:, pl.ds(pl.multiple_of(slot * width, width), width)]
        if piece is not None:
            copies.append(pltpu.make_async_copy(piece, dst, sems.at[k]))
            copies[-1].start()
        else:
            ws[:, pl.ds(pl.multiple_of(slot * width, width), width)] = jnp.zeros(
                (ws.shape[0], width), ws.dtype
            )
    for copy in copies:
        copy.wait()
    for out, base in ((send, 2 * width), (keep, 0)):
        for m, hidden in enumerate((near, far)):
            term = jnp.dot(
                hidden[...], ws[:, base : base + 2 * width], preferred_element_type=jnp.float32
            )
            for owner_x in range(2):
                out[owner_x, m] = term[:, owner_x * width : (owner_x + 1) * width].astype(out.dtype)


def down_terms(place, near, far, pieces):
    shape = (2, 2, near.shape[0], pieces[0].shape[1])
    shape = jax.ShapeDtypeStruct(shape, jnp.bfloat16)
    anywhere = pl.BlockSpec(memory_space=pl.ANY)
    return pl.pallas_call(
        down_kernel,
        in_specs=[pl.BlockSpec(memory_space=pltpu.SMEM), vmem(), vmem()] + [anywhere] * len(pieces),
        out_specs=[vmem(), vmem()],
        out_shape=[shape, shape],
        scratch_shapes=[
            pltpu.VMEM((pieces[0].shape[0], 4 * pieces[0].shape[1]), jnp.bfloat16),
            pltpu.SemaphoreType.DMA((4,)),
        ],
        compiler_params=room(12),
        name="down_terms",
    )(place, near, far, *pieces)


def last_kernel(place, near, far, piece, keep_in, send_in, keep, send, made, sems):
    sp, tp = place[0], place[1]
    low, high, core = (sp // 2) % 2, sp // 4, tp % 2
    for m, hidden in enumerate((near, far)):
        term = jnp.dot(hidden[...], piece[...], preferred_element_type=jnp.float32)
        made[m] = term.astype(made.dtype)
    leaves = low ^ core ^ 1

    @pl.when(leaves == 0)
    def _():
        pltpu.make_async_copy(made, keep.at[1 - high], sems.at[0]).start()

    @pl.when(leaves != 0)
    def _():
        pltpu.make_async_copy(made, send.at[1 - high], sems.at[0]).start()

    pltpu.make_async_copy(made, keep.at[1 - high], sems.at[0]).wait()


def last_terms(place, near, far, piece, keep, send):
    shape = jax.ShapeDtypeStruct(keep.shape, keep.dtype)
    anywhere = pl.BlockSpec(memory_space=pl.ANY)
    return pl.pallas_call(
        last_kernel,
        in_specs=[pl.BlockSpec(memory_space=pltpu.SMEM)] + [vmem()] * 3 + [anywhere] * 2,
        out_specs=[anywhere] * 2,
        out_shape=[shape, shape],
        scratch_shapes=[
            pltpu.VMEM(keep.shape[1:], keep.dtype),
            pltpu.SemaphoreType.DMA((1,)),
        ],
        input_output_aliases={4: 0, 5: 1},
        compiler_params=room(8),
        name="last_terms",
    )(place, near, far, piece, keep, send)


def reduced(keep, send, x):
    came = swapped(send, tp_mask=1)
    keep_a, send_a, keep_b, send_b = fold(x, keep, came)
    came_b = swapped(send_b, sp_mask=2)
    came_a = swapped(send_a, tp_mask=2)
    keep_a, send_a, keep_b, send_b = refold(x, keep_a, came_a, keep_b, came_b)
    came_a = swapped(send_a, sp_mask=2)
    came_b = swapped(send_b, tp_mask=2)
    add = lambda one, two: one.astype(jnp.float32) + two.astype(jnp.float32)
    return jnp.concatenate([add(keep_a, came_a), add(keep_b, came_b)], axis=1)


def local_heads(came, query_rows, key_rows, value_rows, doc_ids, sink_logit):
    rows = query_rows.shape[0]
    kv_local = key_rows.shape[1] // HD
    heads_local = query_rows.shape[1] // HD
    groups = heads_local // kv_local
    reach = WIN + TAIL
    offset = lax.axis_index("sp") * rows
    at = 4 * HD * WIN // LANES
    wide = lambda lines: jnp.concatenate(
        [lines[i : i + TAIL] for i in range(0, lines.shape[0], TAIL)], axis=1
    )
    q_lines = TAIL * query_rows.shape[1] // LANES
    prev_keys, prev_values = (
        jnp.concatenate([came[i : i + HD], came[i + HD : i + 2 * HD]], axis=1)[:, 2 * WIN - reach :]
        for i in (0, 2 * HD)
    )
    prev_docs = came[at : at + 2].reshape(2 * LANES)[2 * LANES - reach :].astype(jnp.int32)
    at = at + TAIL
    prev_queries = wide(came[at : at + q_lines])
    prev_residual = wide(came[at + q_lines :])
    all_keys = jnp.concatenate([prev_keys, key_rows.T], axis=1).T.reshape(rows + reach, kv_local, HD)
    all_values = jnp.concatenate([prev_values, value_rows.T], axis=1).T
    all_values = all_values.reshape(rows + reach, kv_local, HD)
    all_docs = jnp.concatenate([prev_docs, doc_ids])
    key_pos = offset - reach + jnp.arange(rows + reach, dtype=jnp.int32)
    query_pos = offset - TAIL + jnp.arange(rows + TAIL, dtype=jnp.int32)
    queries = jnp.concatenate([prev_queries, query_rows]).reshape(rows + TAIL, kv_local, groups, HD)
    sink = sink_logit.reshape(kv_local, groups, 1, 1)
    pieces = attend(
        queries, all_keys, all_values, query_pos, key_pos, all_docs[WIN:], all_docs, sink
    )
    return pieces.reshape(rows + TAIL, heads_local * HD), prev_docs, prev_residual


def paired(
    query_rows,
    key_rows,
    value_rows,
    doc_ids,
    sink_logit,
    residual,
    out_proj,
    mix_gain,
    gate_proj,
    value_proj,
    gate_taps,
    value_taps,
    down_proj,
    final_gain,
):
    rows, width = residual.shape
    n_tp = lax.axis_size("tp")
    quarter = rows // n_tp
    share = width // n_tp
    sp, tp = lax.axis_index("sp"), lax.axis_index("tp")
    y, low = sp % 2, (sp // 2) % 2
    x, core = tp // 2, tp % 2
    place = jnp.stack([sp, tp]).astype(jnp.int32)
    one = lambda index: index.astype(jnp.int32)[None]
    low_at, x_at, core_at = one(low), one(x), one(core)

    docs_rows = doc_ids.reshape(rows // LANES, LANES)
    halo = packed(query_rows, key_rows, value_rows, docs_rows, residual)
    came_halo = passed_along(halo, "sp", 1)
    own, other = prepared(low_at, gate_proj, value_proj)
    from_z = [own, swapped(other, 2), swapped(own, 4), swapped(other, 6)]
    up_weights = []
    for piece in from_z:
        up_weights += [piece, swapped(piece, 1)]
    own, other = row_halves(low_at, down_proj)
    down_same = [own, swapped(other, 2), swapped(own, 4), swapped(other, 6)]
    down_far = [swapped(piece, 1) for piece in down_same]

    heads, prev_docs, prev_residual = local_heads(
        came_halo, query_rows, key_rows, value_rows, doc_ids, sink_logit
    )
    docs = jnp.concatenate([prev_docs[-2:], doc_ids])
    flags = jnp.stack([docs[1:-1] == doc_ids, docs[:-2] == doc_ids]).astype(jnp.float32)
    flags = lax.dynamic_slice_in_dim(flags, tp * quarter, quarter, 1)
    flags = jnp.pad(flags, ((0, TAIL - 2), (0, 0)))
    keep, send = project(place, heads, out_proj, quarter)
    came = swapped(send, tp_mask=1)
    keep, send = merge(x_at, keep, came)
    came = swapped(send, tp_mask=2)
    normed = normed_rows(
        place, keep, came, residual, prev_residual, mix_gain[None, :], flags
    )
    near = [normed, swapped(normed, tp_mask=2)]
    near += [swapped(near[0], tp_mask=1), swapped(near[1], tp_mask=1)]
    normed = swapped(normed, sp_mask=2)
    far = [normed, swapped(normed, tp_mask=2)]
    far += [swapped(far[0], tp_mask=1), swapped(far[1], tp_mask=1)]

    cols = gate_proj.shape[1]
    half = cols // 2
    main = half // LANES * LANES
    rest = half - main
    cut = lambda taps, start, size: lax.dynamic_slice_in_dim(taps, start, size, 1)
    mains = [cut(t, low * (cols - main), main) for t in (gate_taps, value_taps)]
    rests = [cut(t, main + low * rest, rest) for t in (gate_taps, value_taps)]
    mains = jnp.stack([t.reshape(TAPS, main // LANES, LANES) for t in mains], axis=2)
    taps = jnp.concatenate([mains.reshape(TAPS, 2 * main), *rests], axis=1)
    taps = jnp.pad(taps, ((0, 8 - TAPS), (0, 0)))

    near, far, own_normed = up_hidden(place, near, far, up_weights, taps, share)
    terms = down_terms(place, near, far, down_same)
    ffn_same = reduced(*terms, x_at)
    terms = down_terms(place, near, far, down_far[:3])
    terms = last_terms(place, near, far, down_far[3], *terms)
    ffn_far = reduced(*terms, x_at)
    ffn_own = jnp.where(
        y == 0,
        jnp.concatenate([ffn_same, ffn_far], axis=1),
        jnp.concatenate([ffn_far, ffn_same], axis=1),
    )
    second_sum = mix_scale * own_normed.astype(jnp.float32) + ffn_own
    row_sum, row_squares = lax.psum(
        (jnp.sum(second_sum, axis=1), jnp.sum(second_sum * second_sum, axis=1)), "tp"
    )
    mean = row_sum / width
    var = row_squares / width - mean * mean
    return (
        (second_sum - mean[:, None]) * lax.rsqrt(var + norm_eps)[:, None] * final_gain[None, :]
    ).astype(jnp.bfloat16)


def on_device(
    query_rows,
    key_rows,
    value_rows,
    doc_ids,
    sink_logit,
    residual,
    out_proj,
    mix_gain,
    gate_proj,
    value_proj,
    gate_taps,
    value_taps,
    down_proj,
    final_gain,
):
    rows = query_rows.shape[0]
    kv_local = key_rows.shape[1] // HD
    heads_local = query_rows.shape[1] // HD
    groups = heads_local // kv_local
    offset = lax.axis_index("sp") * rows
    prev_keys, prev_values, prev_docs = passed_along(
        (key_rows[rows - WIN :], value_rows[rows - WIN :], doc_ids[rows - WIN :]), "sp", 1
    )
    all_keys = jnp.concatenate([prev_keys, key_rows]).reshape(rows + WIN, kv_local, HD)
    all_values = jnp.concatenate([prev_values, value_rows]).reshape(rows + WIN, kv_local, HD)
    all_docs = jnp.concatenate([prev_docs, doc_ids])
    key_pos = offset - WIN + jnp.arange(rows + WIN, dtype=jnp.int32)
    query_pos = offset + jnp.arange(rows, dtype=jnp.int32)
    queries = query_rows.reshape(rows, kv_local, groups, HD)
    sink = sink_logit.reshape(kv_local, groups, 1, 1)
    pieces = attend(queries, all_keys, all_values, query_pos, key_pos, doc_ids, all_docs, sink)
    heads = pieces.reshape(rows, heads_local * HD)
    partial_value = jnp.dot(heads, out_proj, preferred_element_type=jnp.float32)
    width = residual.shape[1]
    share = width // lax.axis_size("tp")
    col_start = lax.axis_index("tp") * share
    attn_total = lax.psum(partial_value.astype(jnp.bfloat16), "tp").astype(jnp.float32)
    first_sum = mix_scale * residual.astype(jnp.float32) + attn_total
    mean = jnp.mean(first_sum, axis=1, keepdims=True)
    var = jnp.mean(jnp.square(first_sum - mean), axis=1, keepdims=True)
    normed = ((first_sum - mean) * lax.rsqrt(var + norm_eps) * mix_gain[None, :]).astype(
        jnp.bfloat16
    )
    normed_own = lax.dynamic_slice_in_dim(normed, col_start, share, 1)
    up_gate = jnp.dot(
        normed,
        lax.all_gather(gate_proj, "sp", axis=0, tiled=True),
        preferred_element_type=jnp.float32,
    )
    up_value = jnp.dot(
        normed,
        lax.all_gather(value_proj, "sp", axis=0, tiled=True),
        preferred_element_type=jnp.float32,
    )
    up_gate = up_gate.astype(jnp.bfloat16)
    up_value = up_value.astype(jnp.bfloat16)
    lag_rows = TAPS - 1
    prev_gate, prev_value = passed_along(
        (up_gate[rows - lag_rows :], up_value[rows - lag_rows :]), "sp", 1
    )
    tail_docs = prev_docs[WIN - lag_rows :]
    conv_gate = depthwise(prev_gate, up_gate, gate_taps, tail_docs, doc_ids)
    conv_value = depthwise(prev_value, up_value, value_taps, tail_docs, doc_ids)
    hidden = (jax.nn.gelu(conv_gate) * conv_value).astype(jnp.bfloat16)
    terms = jnp.dot(
        hidden,
        lax.all_gather(down_proj, "sp", axis=1, tiled=True),
        preferred_element_type=jnp.float32,
    )
    ffn_own = lax.psum_scatter(
        terms.astype(jnp.bfloat16), "tp", scatter_dimension=1, tiled=True
    ).astype(jnp.float32)
    second_sum = mix_scale * normed_own.astype(jnp.float32) + ffn_own
    row_sum, row_squares = lax.psum(
        (jnp.sum(second_sum, axis=1), jnp.sum(second_sum * second_sum, axis=1)), "tp"
    )
    mean = row_sum / width
    var = row_squares / width - mean * mean
    return (
        (second_sum - mean[:, None]) * lax.rsqrt(var + norm_eps)[:, None] * final_gain[None, :]
    ).astype(jnp.bfloat16)


def solution(mesh):
    placed = (
        P("sp", "tp"),
        P("sp", "tp"),
        P("sp", "tp"),
        P("sp"),
        P("tp"),
        P("sp", None),
        P("tp", None),
        P(),
        P("sp", "tp"),
        P("sp", "tp"),
        P(None, "tp"),
        P(None, "tp"),
        P("tp", "sp"),
        P("tp"),
    )
    fits = mesh.shape["sp"] == 2 * mesh.shape["tp"] and mesh.shape["tp"] == 4
    return jax.shard_map(
        paired if fits else on_device,
        mesh=mesh,
        in_specs=placed,
        out_specs=P("sp", "tp"),
        check_vma=False,
    )
```

```python
import functools
import math

import jax
import jax.numpy as jnp
from jax import lax
from jax.experimental import pallas as pl
from jax.experimental.pallas import tpu as pltpu
from jax.sharding import PartitionSpec as P


HD = 64
WIN = 128
TAPS = 3
LANES = 128
TAIL = 8
RS_ROOM = 56


mix_scale = math.sqrt(2.0)
norm_eps = 1e-05


def passed_along(block, axis, distance):
    devices = range(lax.axis_size(axis))
    route = [(i - distance, i) for i in devices if i - distance in devices]
    return lax.ppermute(block, axis, route)


def swapped(block, sp_mask=0, tp_mask=0):
    n_sp, n_tp = lax.axis_size("sp"), lax.axis_size("tp")
    if not tp_mask:
        return lax.ppermute(block, "sp", [(i, i ^ sp_mask) for i in range(n_sp)])
    if not sp_mask:
        return lax.ppermute(block, "tp", [(i, i ^ tp_mask) for i in range(n_tp)])
    route = [
        (i * n_tp + j, (i ^ sp_mask) * n_tp + (j ^ tp_mask))
        for i in range(n_sp)
        for j in range(n_tp)
    ]
    return lax.ppermute(block, ("sp", "tp"), route)


def attend(query_block, key_block, value_block, query_pos, key_pos, query_doc, key_doc, sink):
    head_size = query_block.shape[-1]
    scores = jnp.einsum(
        "qkgd,skd->kgqs", query_block, key_block, preferred_element_type=jnp.float32
    ) * head_size ** (-0.5)
    diff = query_pos[:, None] - key_pos[None, :]
    valid = (
        (diff >= 0)
        & (diff < WIN)
        & (query_doc[:, None] == key_doc[None, :])
        & (key_pos[None, :] >= 0)
    )
    scores = jnp.where(valid[None, None], scores, -1e30)
    top = jnp.maximum(jnp.max(scores, axis=-1, keepdims=True), sink)
    weights = jnp.exp(scores - top)
    total = jnp.sum(weights, axis=-1, keepdims=True) + jnp.exp(sink - top)
    probs = (weights / total).astype(jnp.bfloat16)
    out = jnp.einsum("kgqs,skd->qkgd", probs, value_block, preferred_element_type=jnp.float32)
    return out.astype(jnp.bfloat16)


def depthwise(tail, current, taps, tail_docs, docs):
    extended = jnp.concatenate([tail, current])
    ext_docs = jnp.concatenate([tail_docs, docs])
    lag_rows = tail.shape[0]
    count = current.shape[0]
    total = jnp.zeros(current.shape, jnp.float32)
    for lag in range(lag_rows + 1):
        start = lag_rows - lag
        same = (ext_docs[start : start + count] == docs)[:, None]
        rows = extended[start : start + count].astype(jnp.float32)
        total = total + taps[lag][None, :] * jnp.where(same, rows, 0.0)
    return total


def room(mib):
    return pltpu.CompilerParams(vmem_limit_bytes=mib << 20)


def hbm():
    return pl.BlockSpec(memory_space=pltpu.HBM)


def vmem():
    return pl.BlockSpec(memory_space=pltpu.VMEM)


def pack_kernel(queries, keys, values, docs, residual, halo, q, k, v, r, sems):
    rows = queries.shape[0]
    copies = [
        pltpu.make_async_copy(src.at[pl.ds(rows - TAIL, TAIL)], dst, sems.at[i])
        for i, (src, dst) in enumerate(((queries, q), (residual, r)))
    ] + [
        pltpu.make_async_copy(src.at[:, pl.ds(rows - 2 * WIN, 2 * WIN)], dst, sems.at[2 + i])
        for i, (src, dst) in enumerate(((keys, k), (values, v)))
    ]
    for copy in copies:
        copy.start()
    for copy in copies:
        copy.wait()
    at = 0
    last = docs[docs.shape[0] - 2 :, :].astype(jnp.float32)
    last = jnp.concatenate([last, jnp.zeros((TAIL - 2, LANES), jnp.float32)])
    for src in (k, v, last.astype(halo.dtype), q, r):
        for n in range(0, src.shape[1], LANES):
            halo[at : at + src.shape[0], :] = src[:, n : n + LANES]
            at += src.shape[0]


def packed(queries, keys, values, docs, residual):
    lines = 4 * HD * WIN // LANES + TAIL + TAIL * (queries.shape[1] + residual.shape[1]) // LANES
    scratch = [(TAIL, queries.shape[1]), (HD, 2 * WIN), (HD, 2 * WIN), (TAIL, residual.shape[1])]
    return pl.pallas_call(
        pack_kernel,
        in_specs=[hbm(), hbm(), hbm(), vmem(), hbm()],
        out_specs=vmem(),
        out_shape=jax.ShapeDtypeStruct((lines, LANES), jnp.bfloat16),
        scratch_shapes=[pltpu.VMEM(size, jnp.bfloat16) for size in scratch]
        + [pltpu.SemaphoreType.DMA((4,))],
        compiler_params=room(56),
        name="pack",
    )(queries, keys.T, values.T, docs, residual)


def prepare_kernel(which, gates, values, own, other, gate, value, near, far, came, went):
    count, lines, cols = gate.shape
    half = cols // 2
    main = half // LANES * LANES
    rest = half - main
    loads = []
    for i in range(count):
        at = pl.ds(i * lines, lines)
        loads.append(
            [
                pltpu.make_async_copy(src.at[at], dst.at[i], came.at[i, f])
                for f, (src, dst) in enumerate(((gates, gate), (values, value)))
            ]
        )
        for copy in loads[-1]:
            copy.start()

    def emit(i, part, out):
        start = part * (cols - main)
        for n in range(0, main, LANES):
            out[i, :, 2 * n : 2 * n + LANES] = gate[i, :, start + n : start + n + LANES]
            out[i, :, 2 * n + LANES : 2 * n + 2 * LANES] = value[
                i, :, start + n : start + n + LANES
            ]
        left = gate[i, :, main : main + LANES].astype(jnp.float32)
        right = value[i, :, main : main + LANES].astype(jnp.float32)
        if part:
            left = pltpu.roll(left, rest, 1)
        else:
            right = pltpu.roll(right, rest, 1)
        lane = lax.broadcasted_iota(jnp.int32, left.shape, 1)
        out[i, :, 2 * main :] = jnp.where(lane < rest, left, right).astype(out.dtype)

    stores = []
    for i in range(count):
        for copy in loads[i]:
            copy.wait()

        @pl.when(which[0] == 0)
        def _(i=i):
            emit(i, 0, near)
            emit(i, 1, far)

        @pl.when(which[0] != 0)
        def _(i=i):
            emit(i, 1, near)
            emit(i, 0, far)

        for f, (src, dst) in enumerate(((near, own), (far, other))):
            copy = pltpu.make_async_copy(src.at[i], dst.at[pl.ds(i * lines, lines)], went.at[i, f])
            copy.start()
            stores.append(copy)
    for copy in stores:
        copy.wait()


def prepared(which, gate, value):
    count = 4
    shape = jax.ShapeDtypeStruct(gate.shape, gate.dtype)
    cut = pltpu.VMEM((count, gate.shape[0] // count, gate.shape[1]), gate.dtype)
    return pl.pallas_call(
        prepare_kernel,
        in_specs=[pl.BlockSpec(memory_space=pltpu.SMEM), hbm(), hbm()],
        out_specs=[pl.BlockSpec(memory_space=pl.ANY)] * 2,
        out_shape=[shape, shape],
        scratch_shapes=[cut] * 4 + [pltpu.SemaphoreType.DMA((count, 2))] * 2,
        compiler_params=room(56),
        name="prepare",
    )(which, gate, value)


def row_halves_kernel(which, down, own, other, sems):
    rows = down.shape[0]
    half = rows // 2
    main = half // LANES * LANES
    rest = half - main
    for f, out in enumerate((own, other)):
        part = which[0] ^ f
        start = pl.multiple_of(part * (rows - main), 2 * TAIL)
        left = pl.multiple_of(main + part * rest, 2 * TAIL)
        copies = [
            pltpu.make_async_copy(
                down.at[pl.ds(start, main)], out.at[pl.ds(0, main)], sems.at[f, 0]
            ),
            pltpu.make_async_copy(
                down.at[pl.ds(left, rest)], out.at[pl.ds(main, rest)], sems.at[f, 1]
            ),
        ]
        for copy in copies:
            copy.start()
    for f, out in enumerate((own, other)):
        pltpu.make_async_copy(
            down.at[pl.ds(0, main)], out.at[pl.ds(0, main)], sems.at[f, 0]
        ).wait()
        pltpu.make_async_copy(
            down.at[pl.ds(0, rest)], out.at[pl.ds(main, rest)], sems.at[f, 1]
        ).wait()


def row_halves(which, down):
    shape = jax.ShapeDtypeStruct((down.shape[0] // 2, down.shape[1]), down.dtype)
    return pl.pallas_call(
        row_halves_kernel,
        in_specs=[pl.BlockSpec(memory_space=pltpu.SMEM), hbm()],
        out_specs=[vmem(), vmem()],
        out_shape=[shape, shape],
        scratch_shapes=[pltpu.SemaphoreType.DMA((2, 2))],
        compiler_params=room(56),
        name="row_halves",
    )(which, down)


def up_kernel(place, *refs, pieces, quarter):
    chunks = (refs[:4], refs[4:8])
    weights = refs[8 : 8 + pieces]
    taps, *hiddens, own_normed, xs, ws, up, flags, same, sems = refs[8 + pieces :]
    sp, tp = place[0], place[1]
    x, core = tp // 2, tp % 2
    piece_rows = weights[0].shape[0]
    block = 4 * quarter

    def rows_in(m):
        copies = []
        for i, chunk in enumerate(chunks[m]):
            number = (x ^ (i % 2)) * 2 + (core ^ (i // 2))
            parts = (
                (
                    chunk.at[pl.ds(TAIL, quarter)],
                    xs.at[m, pl.ds(pl.multiple_of(TAIL + number * quarter, TAIL), quarter)],
                ),
                (chunk.at[pl.ds(0, TAIL), pl.ds(0, LANES)], flags.at[m, number]),
            )
            for f, (src, dst) in enumerate(parts):
                copies.append(pltpu.make_async_copy(src, dst, sems.at[m, 2 * i + f]))
                copies[-1].start()

            @pl.when(number == 0)
            def _(chunk=chunk):
                pltpu.make_async_copy(
                    chunk.at[pl.ds(0, TAIL)], xs.at[m, pl.ds(0, TAIL)], sems.at[m, 8]
                ).start()

        copies.append(
            pltpu.make_async_copy(
                chunks[m][0].at[pl.ds(0, TAIL)], xs.at[m, pl.ds(0, TAIL)], sems.at[m, 8]
            )
        )
        return copies

    near = rows_in(0)
    loads = []
    for j in range(pieces):
        dst = ws.at[pl.ds(pl.multiple_of((sp ^ j) * piece_rows, piece_rows), piece_rows)]
        loads.append(pltpu.make_async_copy(weights[j], dst, sems.at[2, j]))
        loads[-1].start()
    far = rows_in(1)
    half = ws.shape[1] // 2
    main = half // LANES * LANES
    rest = half - main
    pair = 2 * LANES
    sub = 64
    line = lax.broadcasted_iota(jnp.int32, (quarter, quarter), 0)
    diagonal = line == lax.broadcasted_iota(jnp.int32, (quarter, quarter), 1)
    ones = jnp.ones((quarter, LANES), jnp.bfloat16)

    def spread_flags(m):
        for i in range(4):
            rows = flags[m, i].astype(jnp.float32)
            for lag in range(2):
                spread = jnp.where(diagonal, rows[lag : lag + 1], 0.0).astype(jnp.bfloat16)
                same[lag, i * quarter : (i + 1) * quarter] = jnp.dot(
                    spread, ones, preferred_element_type=jnp.float32
                )

    def conv(rows, start, tap, one, two):
        lag1 = rows[TAIL - 1 : TAIL - 1 + sub, start : start + LANES]
        lag2 = rows[TAIL - 2 : TAIL - 2 + sub, start : start + LANES]
        return (
            tap[0:1] * rows[TAIL:, start : start + LANES]
            + tap[1:2] * jnp.where(one > 0, lag1, 0.0)
            + tap[2:3] * jnp.where(two > 0, lag2, 0.0)
        )

    def gelu(v):
        inner = v * (math.sqrt(2.0 / math.pi) + (0.044715 * math.sqrt(2.0 / math.pi)) * (v * v))
        return (0.5 * v) * (1.0 + jnp.tanh(inner))

    def mix(hidden):
        def step(i, _):
            at = pl.ds(pl.multiple_of(i * sub, sub), sub)
            reach = pl.ds(pl.multiple_of(i * sub, sub), sub + TAIL)
            one, two = same[0, at, :], same[1, at, :]
            for n in range(0, main, LANES):
                rows = up[reach, 2 * n : 2 * n + pair]
                tap = taps[:, 2 * n : 2 * n + pair]
                h = gelu(conv(rows, 0, tap[:, :LANES], one, two))
                h = h * conv(rows, LANES, tap[:, LANES:], one, two)
                hidden[at, n : n + LANES] = h.astype(hidden.dtype)
            mixed = conv(up[reach, 2 * main :], 0, taps[:, 2 * main :], one, two)
            h = gelu(mixed) * pltpu.roll(mixed, rest, 1)
            hidden[at, main:] = h[:, :rest].astype(hidden.dtype)
            return 0

        lax.fori_loop(0, block // sub, step, 0)

    depth = ws.shape[0] // 2
    for copy in (*near, *loads[: pieces // 2]):
        copy.wait()
    first = sp // (pieces // 2)
    at = pl.ds(pl.multiple_of(first * depth, depth), depth)
    up[...] = jnp.dot(xs[0, :, at], ws[at, :], preferred_element_type=jnp.float32)
    spread_flags(0)
    for copy in loads[pieces // 2 :]:
        copy.wait()
    at = pl.ds(pl.multiple_of((1 - first) * depth, depth), depth)
    up[...] += jnp.dot(xs[0, :, at], ws[at, :], preferred_element_type=jnp.float32)
    mix(hiddens[0])
    for copy in far:
        copy.wait()
    spread_flags(1)
    up[...] = jnp.dot(xs[1], ws[...], preferred_element_type=jnp.float32)
    mix(hiddens[1])
    share = own_normed.shape[1]
    own_normed[...] = xs[0, TAIL:, pl.ds(pl.multiple_of(tp * share, share), share)]


def up_hidden(place, near, far, weights, taps, share):
    quarter = near[0].shape[0] - TAIL
    width = near[0].shape[1]
    block = 4 * quarter
    cols = weights[0].shape[1]
    anywhere = pl.BlockSpec(memory_space=pl.ANY)
    return pl.pallas_call(
        functools.partial(up_kernel, pieces=len(weights), quarter=quarter),
        in_specs=[pl.BlockSpec(memory_space=pltpu.SMEM)]
        + [anywhere] * (8 + len(weights))
        + [vmem()],
        out_specs=[vmem()] * 3,
        out_shape=[
            jax.ShapeDtypeStruct((block, cols // 2), jnp.bfloat16),
            jax.ShapeDtypeStruct((block, cols // 2), jnp.bfloat16),
            jax.ShapeDtypeStruct((block, share), jnp.bfloat16),
        ],
        scratch_shapes=[
            pltpu.VMEM((2, block + TAIL, width), jnp.bfloat16),
            pltpu.VMEM((width, cols), jnp.bfloat16),
            pltpu.VMEM((block + TAIL, cols), jnp.float32),
            pltpu.VMEM((2, 4, TAIL, LANES), jnp.bfloat16),
            pltpu.VMEM((2, block, LANES), jnp.float32),
            pltpu.SemaphoreType.DMA((3, max(9, len(weights)))),
        ],
        compiler_params=room(24),
        name="up_hidden",
    )(place, *near, *far, *weights, taps)


def project_kernel(place, heads, weights, keep, send, left, right, made, came, went, *, quarter):
    core = place[1] % 2
    count = right.shape[0]
    wide = right.shape[2]
    loads = [pltpu.make_async_copy(heads, left, came.at[count])]
    for n in range(count):
        cols = pl.ds(n * wide, wide)
        loads.append(pltpu.make_async_copy(weights.at[:, cols], right.at[n], came.at[n]))
    for copy in loads:
        copy.start()
    loads[0].wait()
    stores = []
    for n in range(count):
        loads[1 + n].wait()
        term = jnp.dot(left[...], right[n], preferred_element_type=jnp.float32)
        made[n] = term.astype(made.dtype)
        for f, (out, owner) in enumerate(((send, 1 - core), (keep, core))):
            for x in range(2):
                start = pl.multiple_of((2 * x + owner) * quarter, quarter)
                copy = pltpu.make_async_copy(
                    made.at[n, pl.ds(start, quarter + TAIL)],
                    out.at[x, :, pl.ds(n * wide, wide)],
                    went.at[n, 2 * f + x],
                )
                copy.start()
                stores.append(copy)
    for copy in stores:
        copy.wait()


def project(place, heads, weights, quarter):
    count, rows = 4, heads.shape[0]
    depth, width = weights.shape
    shape = jax.ShapeDtypeStruct((2, quarter + TAIL, width), jnp.bfloat16)
    anywhere = pl.BlockSpec(memory_space=pl.ANY)
    return pl.pallas_call(
        functools.partial(project_kernel, quarter=quarter),
        in_specs=[pl.BlockSpec(memory_space=pltpu.SMEM), anywhere, anywhere],
        out_specs=[anywhere, anywhere],
        out_shape=[shape, shape],
        scratch_shapes=[
            pltpu.VMEM((rows, depth), jnp.bfloat16),
            pltpu.VMEM((count, depth, width // count), jnp.bfloat16),
            pltpu.VMEM((count, rows, width // count), jnp.bfloat16),
            pltpu.SemaphoreType.DMA((count + 1,)),
            pltpu.SemaphoreType.DMA((count, 4)),
        ],
        compiler_params=room(RS_ROOM),
        name="project",
    )(place, heads, weights)


def merge_kernel(which, first, second, keep, send):
    own = which[0]
    for out, part in ((send, 1 - own), (keep, own)):
        out[...] = first[part] + second[part]


def merge(which, first, second):
    shape = jax.ShapeDtypeStruct(first.shape[1:], jnp.bfloat16)
    return pl.pallas_call(
        merge_kernel,
        in_specs=[pl.BlockSpec(memory_space=pltpu.SMEM), vmem(), vmem()],
        out_specs=[vmem(), vmem()],
        out_shape=[shape, shape],
        compiler_params=room(RS_ROOM),
        name="merge",
    )(which, first, second)


def fold_kernel(which, first, second, keep_a, send_a, keep_b, send_b):
    own = which[0]
    half = first.shape[3] // 2
    for l in range(2):
        for out, part in ((send_a, 1 - own), (keep_a, own)):
            out[l] = first[part, l, :, :half] + second[part, l, :, :half]
    for x in range(2):
        for out, part in ((send_b, 1), (keep_b, 0)):
            out[x] = first[x, part, :, half:] + second[x, part, :, half:]


def fold(which, first, second):
    _, _, rows, cols = first.shape
    shape = jax.ShapeDtypeStruct((2, rows, cols // 2), jnp.bfloat16)
    return pl.pallas_call(
        fold_kernel,
        in_specs=[pl.BlockSpec(memory_space=pltpu.SMEM), vmem(), vmem()],
        out_specs=[vmem()] * 4,
        out_shape=[shape] * 4,
        compiler_params=room(4),
        name="fold",
    )(which, first, second)


def refold_kernel(which, keep_a, came_a, keep_b, came_b, stay_a, send_a, stay_b, send_b):
    own = which[0]
    stay_a[...] = keep_a[0] + came_a[0]
    send_a[...] = keep_a[1] + came_a[1]
    stay_b[...] = keep_b[own] + came_b[own]
    send_b[...] = keep_b[1 - own] + came_b[1 - own]


def refold(which, *arrays):
    shape = jax.ShapeDtypeStruct(arrays[0].shape[1:], jnp.bfloat16)
    return pl.pallas_call(
        refold_kernel,
        in_specs=[pl.BlockSpec(memory_space=pltpu.SMEM)] + [vmem()] * 4,
        out_specs=[vmem()] * 4,
        out_shape=[shape] * 4,
        compiler_params=room(4),
        name="refold",
    )(which, *arrays)


def norm_kernel(place, first, second, residual, before, gain, flags, out, base, sems):
    tp = place[1]
    rows = first.shape[0]
    quarter = rows - TAIL
    start = pl.multiple_of(tp * quarter, quarter)
    body = pltpu.make_async_copy(
        residual.at[pl.ds(start, quarter)], base.at[pl.ds(TAIL, quarter)], sems.at[0]
    )
    body.start()
    top = base.at[pl.ds(0, TAIL)]

    @pl.when(tp == 0)
    def _():
        pltpu.make_async_copy(before, top, sems.at[1]).start()

    @pl.when(tp != 0)
    def _():
        at = pl.multiple_of(jnp.maximum(start - TAIL, 0), TAIL)
        pltpu.make_async_copy(residual.at[pl.ds(at, TAIL)], top, sems.at[1]).start()

    pltpu.make_async_copy(before, top, sems.at[1]).wait()
    body.wait()
    group = 64
    for r in range(0, rows, group):
        at = slice(r, min(r + group, rows))
        total = first[at].astype(jnp.float32) + second[at].astype(jnp.float32)
        total = mix_scale * base[at].astype(jnp.float32) + total
        mean = jnp.mean(total, axis=1, keepdims=True)
        var = jnp.mean(total * total, axis=1, keepdims=True) - mean * mean
        out[at] = ((total - mean) * lax.rsqrt(var + norm_eps) * gain[...]).astype(out.dtype)
    line = lax.broadcasted_iota(jnp.int32, (TAIL, LANES), 0)
    rows_of = out[:TAIL, :LANES].astype(jnp.float32)
    out[:TAIL, :LANES] = jnp.where(line < 2, flags[...], rows_of).astype(out.dtype)


def normed_rows(place, first, second, residual, before, gain, flags):
    return pl.pallas_call(
        norm_kernel,
        in_specs=[pl.BlockSpec(memory_space=pltpu.SMEM), vmem(), vmem(), hbm(), hbm(), vmem(), vmem()],
        out_specs=vmem(),
        out_shape=jax.ShapeDtypeStruct(first.shape, jnp.bfloat16),
        scratch_shapes=[pltpu.VMEM(first.shape, jnp.bfloat16), pltpu.SemaphoreType.DMA((2,))],
        compiler_params=room(RS_ROOM),
        name="normed_rows",
    )(place, first, second, residual, before, gain, flags)


def down_kernel(place, near, far, *refs):
    *pieces, keep, send, ws, sems = refs
    if len(pieces) == 3:
        pieces.append(None)
    sp, tp = place[0], place[1]
    low, high, core = (sp // 2) % 2, sp // 4, tp % 2
    width = pieces[0].shape[1]
    copies = []
    for k, piece in enumerate(pieces):
        slot = 2 * (low ^ (k % 2) ^ core) + (high ^ (k // 2))
        dst = ws.at[:, pl.ds(pl.multiple_of(slot * width, width), width)]
        if piece is not None:
            copies.append(pltpu.make_async_copy(piece, dst, sems.at[k]))
            copies[-1].start()
        else:
            ws[:, pl.ds(pl.multiple_of(slot * width, width), width)] = jnp.zeros(
                (ws.shape[0], width), ws.dtype
            )
    for copy in copies:
        copy.wait()
    for out, base in ((send, 2 * width), (keep, 0)):
        for m, hidden in enumerate((near, far)):
            term = jnp.dot(
                hidden[...], ws[:, base : base + 2 * width], preferred_element_type=jnp.float32
            )
            for owner_x in range(2):
                out[owner_x, m] = term[:, owner_x * width : (owner_x + 1) * width].astype(out.dtype)


def down_terms(place, near, far, pieces):
    shape = (2, 2, near.shape[0], pieces[0].shape[1])
    shape = jax.ShapeDtypeStruct(shape, jnp.bfloat16)
    anywhere = pl.BlockSpec(memory_space=pl.ANY)
    return pl.pallas_call(
        down_kernel,
        in_specs=[pl.BlockSpec(memory_space=pltpu.SMEM), vmem(), vmem()] + [anywhere] * len(pieces),
        out_specs=[vmem(), vmem()],
        out_shape=[shape, shape],
        scratch_shapes=[
            pltpu.VMEM((pieces[0].shape[0], 4 * pieces[0].shape[1]), jnp.bfloat16),
            pltpu.SemaphoreType.DMA((4,)),
        ],
        compiler_params=room(12),
        name="down_terms",
    )(place, near, far, *pieces)


def last_kernel(place, near, far, piece, keep_in, send_in, keep, send, made, sems):
    sp, tp = place[0], place[1]
    low, high, core = (sp // 2) % 2, sp // 4, tp % 2
    for m, hidden in enumerate((near, far)):
        term = jnp.dot(hidden[...], piece[...], preferred_element_type=jnp.float32)
        made[m] = term.astype(made.dtype)
    leaves = low ^ core ^ 1

    @pl.when(leaves == 0)
    def _():
        pltpu.make_async_copy(made, keep.at[1 - high], sems.at[0]).start()

    @pl.when(leaves != 0)
    def _():
        pltpu.make_async_copy(made, send.at[1 - high], sems.at[0]).start()

    pltpu.make_async_copy(made, keep.at[1 - high], sems.at[0]).wait()


def last_terms(place, near, far, piece, keep, send):
    shape = jax.ShapeDtypeStruct(keep.shape, keep.dtype)
    anywhere = pl.BlockSpec(memory_space=pl.ANY)
    return pl.pallas_call(
        last_kernel,
        in_specs=[pl.BlockSpec(memory_space=pltpu.SMEM)] + [vmem()] * 3 + [anywhere] * 2,
        out_specs=[anywhere] * 2,
        out_shape=[shape, shape],
        scratch_shapes=[
            pltpu.VMEM(keep.shape[1:], keep.dtype),
            pltpu.SemaphoreType.DMA((1,)),
        ],
        input_output_aliases={4: 0, 5: 1},
        compiler_params=room(8),
        name="last_terms",
    )(place, near, far, piece, keep, send)


def reduced(keep, send, x):
    came = swapped(send, tp_mask=1)
    keep_a, send_a, keep_b, send_b = fold(x, keep, came)
    came_b = swapped(send_b, sp_mask=2)
    came_a = swapped(send_a, tp_mask=2)
    keep_a, send_a, keep_b, send_b = refold(x, keep_a, came_a, keep_b, came_b)
    came_a = swapped(send_a, sp_mask=2)
    came_b = swapped(send_b, tp_mask=2)
    add = lambda one, two: one.astype(jnp.float32) + two.astype(jnp.float32)
    return jnp.concatenate([add(keep_a, came_a), add(keep_b, came_b)], axis=1)


def local_heads(came, query_rows, key_rows, value_rows, doc_ids, sink_logit):
    rows = query_rows.shape[0]
    kv_local = key_rows.shape[1] // HD
    heads_local = query_rows.shape[1] // HD
    groups = heads_local // kv_local
    reach = WIN + TAIL
    offset = lax.axis_index("sp") * rows
    at = 4 * HD * WIN // LANES
    wide = lambda lines: jnp.concatenate(
        [lines[i : i + TAIL] for i in range(0, lines.shape[0], TAIL)], axis=1
    )
    q_lines = TAIL * query_rows.shape[1] // LANES
    prev_keys, prev_values = (
        jnp.concatenate([came[i : i + HD], came[i + HD : i + 2 * HD]], axis=1)[:, 2 * WIN - reach :]
        for i in (0, 2 * HD)
    )
    prev_docs = came[at : at + 2].reshape(2 * LANES)[2 * LANES - reach :].astype(jnp.int32)
    at = at + TAIL
    prev_queries = wide(came[at : at + q_lines])
    prev_residual = wide(came[at + q_lines :])
    all_keys = jnp.concatenate([prev_keys, key_rows.T], axis=1).T.reshape(rows + reach, kv_local, HD)
    all_values = jnp.concatenate([prev_values, value_rows.T], axis=1).T
    all_values = all_values.reshape(rows + reach, kv_local, HD)
    all_docs = jnp.concatenate([prev_docs, doc_ids])
    key_pos = offset - reach + jnp.arange(rows + reach, dtype=jnp.int32)
    query_pos = offset - TAIL + jnp.arange(rows + TAIL, dtype=jnp.int32)
    queries = jnp.concatenate([prev_queries, query_rows]).reshape(rows + TAIL, kv_local, groups, HD)
    sink = sink_logit.reshape(kv_local, groups, 1, 1)
    pieces = attend(
        queries, all_keys, all_values, query_pos, key_pos, all_docs[WIN:], all_docs, sink
    )
    return pieces.reshape(rows + TAIL, heads_local * HD), prev_docs, prev_residual


def paired(
    query_rows,
    key_rows,
    value_rows,
    doc_ids,
    sink_logit,
    residual,
    out_proj,
    mix_gain,
    gate_proj,
    value_proj,
    gate_taps,
    value_taps,
    down_proj,
    final_gain,
):
    rows, width = residual.shape
    n_tp = lax.axis_size("tp")
    quarter = rows // n_tp
    share = width // n_tp
    sp, tp = lax.axis_index("sp"), lax.axis_index("tp")
    y, low = sp % 2, (sp // 2) % 2
    x, core = tp // 2, tp % 2
    place = jnp.stack([sp, tp]).astype(jnp.int32)
    one = lambda index: index.astype(jnp.int32)[None]
    low_at, x_at, core_at = one(low), one(x), one(core)

    docs_rows = doc_ids.reshape(rows // LANES, LANES)
    halo = packed(query_rows, key_rows, value_rows, docs_rows, residual)
    came_halo = passed_along(halo, "sp", 1)
    own, other = prepared(low_at, gate_proj, value_proj)
    from_z = [own, swapped(other, 2), swapped(own, 4), swapped(other, 6)]
    up_weights = []
    for piece in from_z:
        up_weights += [piece, swapped(piece, 1)]
    own, other = row_halves(low_at, down_proj)
    down_same = [own, swapped(other, 2), swapped(own, 4), swapped(other, 6)]
    down_far = [swapped(piece, 1) for piece in down_same]

    heads, prev_docs, prev_residual = local_heads(
        came_halo, query_rows, key_rows, value_rows, doc_ids, sink_logit
    )
    docs = jnp.concatenate([prev_docs[-2:], doc_ids])
    flags = jnp.stack([docs[1:-1] == doc_ids, docs[:-2] == doc_ids]).astype(jnp.float32)
    flags = lax.dynamic_slice_in_dim(flags, tp * quarter, quarter, 1)
    flags = jnp.pad(flags, ((0, TAIL - 2), (0, 0)))
    keep, send = project(place, heads, out_proj, quarter)
    came = swapped(send, tp_mask=1)
    keep, send = merge(x_at, keep, came)
    came = swapped(send, tp_mask=2)
    normed = normed_rows(
        place, keep, came, residual, prev_residual, mix_gain[None, :], flags
    )
    near = [normed, swapped(normed, tp_mask=2)]
    near += [swapped(near[0], tp_mask=1), swapped(near[1], tp_mask=1)]
    normed = swapped(normed, sp_mask=2)
    far = [normed, swapped(normed, tp_mask=2)]
    far += [swapped(far[0], tp_mask=1), swapped(far[1], tp_mask=1)]

    cols = gate_proj.shape[1]
    half = cols // 2
    main = half // LANES * LANES
    rest = half - main
    cut = lambda taps, start, size: lax.dynamic_slice_in_dim(taps, start, size, 1)
    mains = [cut(t, low * (cols - main), main) for t in (gate_taps, value_taps)]
    rests = [cut(t, main + low * rest, rest) for t in (gate_taps, value_taps)]
    mains = jnp.stack([t.reshape(TAPS, main // LANES, LANES) for t in mains], axis=2)
    taps = jnp.concatenate([mains.reshape(TAPS, 2 * main), *rests], axis=1)
    taps = jnp.pad(taps, ((0, 8 - TAPS), (0, 0)))

    near, far, own_normed = up_hidden(place, near, far, up_weights, taps, share)
    terms = down_terms(place, near, far, down_same)
    ffn_same = reduced(*terms, x_at)
    terms = down_terms(place, near, far, down_far[:3])
    terms = last_terms(place, near, far, down_far[3], *terms)
    ffn_far = reduced(*terms, x_at)
    ffn_own = jnp.where(
        y == 0,
        jnp.concatenate([ffn_same, ffn_far], axis=1),
        jnp.concatenate([ffn_far, ffn_same], axis=1),
    )
    second_sum = mix_scale * own_normed.astype(jnp.float32) + ffn_own
    row_sum, row_squares = lax.psum(
        (jnp.sum(second_sum, axis=1), jnp.sum(second_sum * second_sum, axis=1)), "tp"
    )
    mean = row_sum / width
    var = row_squares / width - mean * mean
    return (
        (second_sum - mean[:, None]) * lax.rsqrt(var + norm_eps)[:, None] * final_gain[None, :]
    ).astype(jnp.bfloat16)


def on_device(
    query_rows,
    key_rows,
    value_rows,
    doc_ids,
    sink_logit,
    residual,
    out_proj,
    mix_gain,
    gate_proj,
    value_proj,
    gate_taps,
    value_taps,
    down_proj,
    final_gain,
):
    rows = query_rows.shape[0]
    kv_local = key_rows.shape[1] // HD
    heads_local = query_rows.shape[1] // HD
    groups = heads_local // kv_local
    offset = lax.axis_index("sp") * rows
    prev_keys, prev_values, prev_docs = passed_along(
        (key_rows[rows - WIN :], value_rows[rows - WIN :], doc_ids[rows - WIN :]), "sp", 1
    )
    all_keys = jnp.concatenate([prev_keys, key_rows]).reshape(rows + WIN, kv_local, HD)
    all_values = jnp.concatenate([prev_values, value_rows]).reshape(rows + WIN, kv_local, HD)
    all_docs = jnp.concatenate([prev_docs, doc_ids])
    key_pos = offset - WIN + jnp.arange(rows + WIN, dtype=jnp.int32)
    query_pos = offset + jnp.arange(rows, dtype=jnp.int32)
    queries = query_rows.reshape(rows, kv_local, groups, HD)
    sink = sink_logit.reshape(kv_local, groups, 1, 1)
    pieces = attend(queries, all_keys, all_values, query_pos, key_pos, doc_ids, all_docs, sink)
    heads = pieces.reshape(rows, heads_local * HD)
    partial_value = jnp.dot(heads, out_proj, preferred_element_type=jnp.float32)
    width = residual.shape[1]
    share = width // lax.axis_size("tp")
    col_start = lax.axis_index("tp") * share
    attn_total = lax.psum(partial_value.astype(jnp.bfloat16), "tp").astype(jnp.float32)
    first_sum = mix_scale * residual.astype(jnp.float32) + attn_total
    mean = jnp.mean(first_sum, axis=1, keepdims=True)
    var = jnp.mean(jnp.square(first_sum - mean), axis=1, keepdims=True)
    normed = ((first_sum - mean) * lax.rsqrt(var + norm_eps) * mix_gain[None, :]).astype(
        jnp.bfloat16
    )
    normed_own = lax.dynamic_slice_in_dim(normed, col_start, share, 1)
    up_gate = jnp.dot(
        normed,
        lax.all_gather(gate_proj, "sp", axis=0, tiled=True),
        preferred_element_type=jnp.float32,
    )
    up_value = jnp.dot(
        normed,
        lax.all_gather(value_proj, "sp", axis=0, tiled=True),
        preferred_element_type=jnp.float32,
    )
    up_gate = up_gate.astype(jnp.bfloat16)
    up_value = up_value.astype(jnp.bfloat16)
    lag_rows = TAPS - 1
    prev_gate, prev_value = passed_along(
        (up_gate[rows - lag_rows :], up_value[rows - lag_rows :]), "sp", 1
    )
    tail_docs = prev_docs[WIN - lag_rows :]
    conv_gate = depthwise(prev_gate, up_gate, gate_taps, tail_docs, doc_ids)
    conv_value = depthwise(prev_value, up_value, value_taps, tail_docs, doc_ids)
    hidden = (jax.nn.gelu(conv_gate) * conv_value).astype(jnp.bfloat16)
    terms = jnp.dot(
        hidden,
        lax.all_gather(down_proj, "sp", axis=1, tiled=True),
        preferred_element_type=jnp.float32,
    )
    ffn_own = lax.psum_scatter(
        terms.astype(jnp.bfloat16), "tp", scatter_dimension=1, tiled=True
    ).astype(jnp.float32)
    second_sum = mix_scale * normed_own.astype(jnp.float32) + ffn_own
    row_sum, row_squares = lax.psum(
        (jnp.sum(second_sum, axis=1), jnp.sum(second_sum * second_sum, axis=1)), "tp"
    )
    mean = row_sum / width
    var = row_squares / width - mean * mean
    return (
        (second_sum - mean[:, None]) * lax.rsqrt(var + norm_eps)[:, None] * final_gain[None, :]
    ).astype(jnp.bfloat16)


def solution(mesh):
    placed = (
        P("sp", "tp"),
        P("sp", "tp"),
        P("sp", "tp"),
        P("sp"),
        P("tp"),
        P("sp", None),
        P("tp", None),
        P(),
        P("sp", "tp"),
        P("sp", "tp"),
        P(None, "tp"),
        P(None, "tp"),
        P("tp", "sp"),
        P("tp"),
    )
    fits = mesh.shape["sp"] == 2 * mesh.shape["tp"] and mesh.shape["tp"] == 4
    return jax.shard_map(
        paired if fits else on_device,
        mesh=mesh,
        in_specs=placed,
        out_specs=P("sp", "tp"),
        check_vma=False,
    )
```

```python
import functools
import math

import jax
import jax.numpy as jnp
from jax import lax
from jax.experimental import pallas as pl
from jax.experimental.pallas import tpu as pltpu
from jax.sharding import PartitionSpec as P


HD = 64
WIN = 128
TAPS = 3
LANES = 128
TAIL = 8
RS_ROOM = 56


mix_scale = math.sqrt(2.0)
norm_eps = 1e-05


def passed_along(block, axis, distance):
    devices = range(lax.axis_size(axis))
    route = [(i - distance, i) for i in devices if i - distance in devices]
    return lax.ppermute(block, axis, route)


def swapped(block, sp_mask=0, tp_mask=0):
    n_sp, n_tp = lax.axis_size("sp"), lax.axis_size("tp")
    if not tp_mask:
        return lax.ppermute(block, "sp", [(i, i ^ sp_mask) for i in range(n_sp)])
    if not sp_mask:
        return lax.ppermute(block, "tp", [(i, i ^ tp_mask) for i in range(n_tp)])
    route = [
        (i * n_tp + j, (i ^ sp_mask) * n_tp + (j ^ tp_mask))
        for i in range(n_sp)
        for j in range(n_tp)
    ]
    return lax.ppermute(block, ("sp", "tp"), route)


def attend(query_block, key_block, value_block, query_pos, key_pos, query_doc, key_doc, sink):
    head_size = query_block.shape[-1]
    scores = jnp.einsum(
        "qkgd,skd->kgqs", query_block, key_block, preferred_element_type=jnp.float32
    ) * head_size ** (-0.5)
    diff = query_pos[:, None] - key_pos[None, :]
    valid = (
        (diff >= 0)
        & (diff < WIN)
        & (query_doc[:, None] == key_doc[None, :])
        & (key_pos[None, :] >= 0)
    )
    scores = jnp.where(valid[None, None], scores, -1e30)
    top = jnp.maximum(jnp.max(scores, axis=-1, keepdims=True), sink)
    weights = jnp.exp(scores - top)
    total = jnp.sum(weights, axis=-1, keepdims=True) + jnp.exp(sink - top)
    probs = (weights / total).astype(jnp.bfloat16)
    out = jnp.einsum("kgqs,skd->qkgd", probs, value_block, preferred_element_type=jnp.float32)
    return out.astype(jnp.bfloat16)


def depthwise(tail, current, taps, tail_docs, docs):
    extended = jnp.concatenate([tail, current])
    ext_docs = jnp.concatenate([tail_docs, docs])
    lag_rows = tail.shape[0]
    count = current.shape[0]
    total = jnp.zeros(current.shape, jnp.float32)
    for lag in range(lag_rows + 1):
        start = lag_rows - lag
        same = (ext_docs[start : start + count] == docs)[:, None]
        rows = extended[start : start + count].astype(jnp.float32)
        total = total + taps[lag][None, :] * jnp.where(same, rows, 0.0)
    return total


def room(mib):
    return pltpu.CompilerParams(vmem_limit_bytes=mib << 20)


def hbm():
    return pl.BlockSpec(memory_space=pltpu.HBM)


def vmem():
    return pl.BlockSpec(memory_space=pltpu.VMEM)


def pack_kernel(queries, keys, values, docs, residual, halo, q, k, v, r, sems):
    rows = queries.shape[0]
    copies = [
        pltpu.make_async_copy(src.at[pl.ds(rows - TAIL, TAIL)], dst, sems.at[i])
        for i, (src, dst) in enumerate(((queries, q), (residual, r)))
    ] + [
        pltpu.make_async_copy(src.at[:, pl.ds(rows - 2 * WIN, 2 * WIN)], dst, sems.at[2 + i])
        for i, (src, dst) in enumerate(((keys, k), (values, v)))
    ]
    for copy in copies:
        copy.start()
    for copy in copies:
        copy.wait()
    at = 0
    last = docs[docs.shape[0] - 2 :, :].astype(jnp.float32)
    last = jnp.concatenate([last, jnp.zeros((TAIL - 2, LANES), jnp.float32)])
    for src in (k, v, last.astype(halo.dtype), q, r):
        for n in range(0, src.shape[1], LANES):
            halo[at : at + src.shape[0], :] = src[:, n : n + LANES]
            at += src.shape[0]


def packed(queries, keys, values, docs, residual):
    lines = 4 * HD * WIN // LANES + TAIL + TAIL * (queries.shape[1] + residual.shape[1]) // LANES
    scratch = [(TAIL, queries.shape[1]), (HD, 2 * WIN), (HD, 2 * WIN), (TAIL, residual.shape[1])]
    return pl.pallas_call(
        pack_kernel,
        in_specs=[hbm(), hbm(), hbm(), vmem(), hbm()],
        out_specs=vmem(),
        out_shape=jax.ShapeDtypeStruct((lines, LANES), jnp.bfloat16),
        scratch_shapes=[pltpu.VMEM(size, jnp.bfloat16) for size in scratch]
        + [pltpu.SemaphoreType.DMA((4,))],
        compiler_params=room(56),
        name="pack",
    )(queries, keys.T, values.T, docs, residual)


def prepare_kernel(which, gates, values, own, other, gate, value, near, far, came, went):
    count, lines, cols = gate.shape
    half = cols // 2
    main = half // LANES * LANES
    rest = half - main
    loads = []
    for i in range(count):
        at = pl.ds(i * lines, lines)
        loads.append(
            [
                pltpu.make_async_copy(src.at[at], dst.at[i], came.at[i, f])
                for f, (src, dst) in enumerate(((gates, gate), (values, value)))
            ]
        )
        for copy in loads[-1]:
            copy.start()

    def emit(i, part, out):
        start = part * (cols - main)
        for n in range(0, main, LANES):
            out[i, :, 2 * n : 2 * n + LANES] = gate[i, :, start + n : start + n + LANES]
            out[i, :, 2 * n + LANES : 2 * n + 2 * LANES] = value[
                i, :, start + n : start + n + LANES
            ]
        left = gate[i, :, main : main + LANES].astype(jnp.float32)
        right = value[i, :, main : main + LANES].astype(jnp.float32)
        if part:
            left = pltpu.roll(left, rest, 1)
        else:
            right = pltpu.roll(right, rest, 1)
        lane = lax.broadcasted_iota(jnp.int32, left.shape, 1)
        out[i, :, 2 * main :] = jnp.where(lane < rest, left, right).astype(out.dtype)

    stores = []
    for i in range(count):
        for copy in loads[i]:
            copy.wait()

        @pl.when(which[0] == 0)
        def _(i=i):
            emit(i, 0, near)
            emit(i, 1, far)

        @pl.when(which[0] != 0)
        def _(i=i):
            emit(i, 1, near)
            emit(i, 0, far)

        for f, (src, dst) in enumerate(((near, own), (far, other))):
            copy = pltpu.make_async_copy(src.at[i], dst.at[pl.ds(i * lines, lines)], went.at[i, f])
            copy.start()
            stores.append(copy)
    for copy in stores:
        copy.wait()


def prepared(which, gate, value):
    count = 4
    shape = jax.ShapeDtypeStruct(gate.shape, gate.dtype)
    cut = pltpu.VMEM((count, gate.shape[0] // count, gate.shape[1]), gate.dtype)
    return pl.pallas_call(
        prepare_kernel,
        in_specs=[pl.BlockSpec(memory_space=pltpu.SMEM), hbm(), hbm()],
        out_specs=[pl.BlockSpec(memory_space=pl.ANY)] * 2,
        out_shape=[shape, shape],
        scratch_shapes=[cut] * 4 + [pltpu.SemaphoreType.DMA((count, 2))] * 2,
        compiler_params=room(56),
        name="prepare",
    )(which, gate, value)


def row_halves_kernel(which, down, own, other, sems):
    rows = down.shape[0]
    half = rows // 2
    main = half // LANES * LANES
    rest = half - main
    for f, out in enumerate((own, other)):
        part = which[0] ^ f
        start = pl.multiple_of(part * (rows - main), 2 * TAIL)
        left = pl.multiple_of(main + part * rest, 2 * TAIL)
        copies = [
            pltpu.make_async_copy(
                down.at[pl.ds(start, main)], out.at[pl.ds(0, main)], sems.at[f, 0]
            ),
            pltpu.make_async_copy(
                down.at[pl.ds(left, rest)], out.at[pl.ds(main, rest)], sems.at[f, 1]
            ),
        ]
        for copy in copies:
            copy.start()
    for f, out in enumerate((own, other)):
        pltpu.make_async_copy(
            down.at[pl.ds(0, main)], out.at[pl.ds(0, main)], sems.at[f, 0]
        ).wait()
        pltpu.make_async_copy(
            down.at[pl.ds(0, rest)], out.at[pl.ds(main, rest)], sems.at[f, 1]
        ).wait()


def row_halves(which, down):
    shape = jax.ShapeDtypeStruct((down.shape[0] // 2, down.shape[1]), down.dtype)
    return pl.pallas_call(
        row_halves_kernel,
        in_specs=[pl.BlockSpec(memory_space=pltpu.SMEM), hbm()],
        out_specs=[vmem(), vmem()],
        out_shape=[shape, shape],
        scratch_shapes=[pltpu.SemaphoreType.DMA((2, 2))],
        compiler_params=room(56),
        name="row_halves",
    )(which, down)


def up_kernel(place, *refs, pieces, quarter):
    chunks = (refs[:4], refs[4:8])
    weights = refs[8 : 8 + pieces]
    taps, *hiddens, own_normed, xs, ws, up, flags, same, sems = refs[8 + pieces :]
    sp, tp = place[0], place[1]
    x, core = tp // 2, tp % 2
    piece_rows = weights[0].shape[0]
    block = 4 * quarter

    def rows_in(m):
        copies = []
        for i, chunk in enumerate(chunks[m]):
            number = (x ^ (i % 2)) * 2 + (core ^ (i // 2))
            parts = (
                (
                    chunk.at[pl.ds(TAIL, quarter)],
                    xs.at[m, pl.ds(pl.multiple_of(TAIL + number * quarter, TAIL), quarter)],
                ),
                (chunk.at[pl.ds(0, TAIL), pl.ds(0, LANES)], flags.at[m, number]),
            )
            for f, (src, dst) in enumerate(parts):
                copies.append(pltpu.make_async_copy(src, dst, sems.at[m, 2 * i + f]))
                copies[-1].start()

            @pl.when(number == 0)
            def _(chunk=chunk):
                pltpu.make_async_copy(
                    chunk.at[pl.ds(0, TAIL)], xs.at[m, pl.ds(0, TAIL)], sems.at[m, 8]
                ).start()

        copies.append(
            pltpu.make_async_copy(
                chunks[m][0].at[pl.ds(0, TAIL)], xs.at[m, pl.ds(0, TAIL)], sems.at[m, 8]
            )
        )
        return copies

    near = rows_in(0)
    loads = []
    for j in range(pieces):
        dst = ws.at[pl.ds(pl.multiple_of((sp ^ j) * piece_rows, piece_rows), piece_rows)]
        loads.append(pltpu.make_async_copy(weights[j], dst, sems.at[2, j]))
        loads[-1].start()
    far = rows_in(1)
    half = ws.shape[1] // 2
    main = half // LANES * LANES
    rest = half - main
    pair = 2 * LANES
    sub = 64
    line = lax.broadcasted_iota(jnp.int32, (quarter, quarter), 0)
    diagonal = line == lax.broadcasted_iota(jnp.int32, (quarter, quarter), 1)
    ones = jnp.ones((quarter, LANES), jnp.bfloat16)

    def spread_flags(m):
        for i in range(4):
            rows = flags[m, i].astype(jnp.float32)
            for lag in range(2):
                spread = jnp.where(diagonal, rows[lag : lag + 1], 0.0).astype(jnp.bfloat16)
                same[lag, i * quarter : (i + 1) * quarter] = jnp.dot(
                    spread, ones, preferred_element_type=jnp.float32
                )

    def conv(rows, start, tap, one, two):
        lag1 = rows[TAIL - 1 : TAIL - 1 + sub, start : start + LANES]
        lag2 = rows[TAIL - 2 : TAIL - 2 + sub, start : start + LANES]
        return (
            tap[0:1] * rows[TAIL:, start : start + LANES]
            + tap[1:2] * jnp.where(one > 0, lag1, 0.0)
            + tap[2:3] * jnp.where(two > 0, lag2, 0.0)
        )

    def gelu(v):
        inner = v * (math.sqrt(2.0 / math.pi) + (0.044715 * math.sqrt(2.0 / math.pi)) * (v * v))
        return (0.5 * v) * (1.0 + jnp.tanh(inner))

    def mix(hidden):
        def step(i, _):
            at = pl.ds(pl.multiple_of(i * sub, sub), sub)
            reach = pl.ds(pl.multiple_of(i * sub, sub), sub + TAIL)
            one, two = same[0, at, :], same[1, at, :]
            for n in range(0, main, LANES):
                rows = up[reach, 2 * n : 2 * n + pair]
                tap = taps[:, 2 * n : 2 * n + pair]
                h = gelu(conv(rows, 0, tap[:, :LANES], one, two))
                h = h * conv(rows, LANES, tap[:, LANES:], one, two)
                hidden[at, n : n + LANES] = h.astype(hidden.dtype)
            mixed = conv(up[reach, 2 * main :], 0, taps[:, 2 * main :], one, two)
            h = gelu(mixed) * pltpu.roll(mixed, rest, 1)
            hidden[at, main:] = h[:, :rest].astype(hidden.dtype)
            return 0

        lax.fori_loop(0, block // sub, step, 0)

    depth = ws.shape[0] // 2
    for copy in (*near, *loads[: pieces // 2]):
        copy.wait()
    first = sp // (pieces // 2)
    at = pl.ds(pl.multiple_of(first * depth, depth), depth)
    up[...] = jnp.dot(xs[0, :, at], ws[at, :], preferred_element_type=jnp.float32)
    spread_flags(0)
    for copy in loads[pieces // 2 :]:
        copy.wait()
    at = pl.ds(pl.multiple_of((1 - first) * depth, depth), depth)
    up[...] += jnp.dot(xs[0, :, at], ws[at, :], preferred_element_type=jnp.float32)
    mix(hiddens[0])
    for copy in far:
        copy.wait()
    spread_flags(1)
    up[...] = jnp.dot(xs[1], ws[...], preferred_element_type=jnp.float32)
    mix(hiddens[1])
    share = own_normed.shape[1]
    own_normed[...] = xs[0, TAIL:, pl.ds(pl.multiple_of(tp * share, share), share)]


def up_hidden(place, near, far, weights, taps, share):
    quarter = near[0].shape[0] - TAIL
    width = near[0].shape[1]
    block = 4 * quarter
    cols = weights[0].shape[1]
    anywhere = pl.BlockSpec(memory_space=pl.ANY)
    return pl.pallas_call(
        functools.partial(up_kernel, pieces=len(weights), quarter=quarter),
        in_specs=[pl.BlockSpec(memory_space=pltpu.SMEM)]
        + [anywhere] * (8 + len(weights))
        + [vmem()],
        out_specs=[vmem()] * 3,
        out_shape=[
            jax.ShapeDtypeStruct((block, cols // 2), jnp.bfloat16),
            jax.ShapeDtypeStruct((block, cols // 2), jnp.bfloat16),
            jax.ShapeDtypeStruct((block, share), jnp.bfloat16),
        ],
        scratch_shapes=[
            pltpu.VMEM((2, block + TAIL, width), jnp.bfloat16),
            pltpu.VMEM((width, cols), jnp.bfloat16),
            pltpu.VMEM((block + TAIL, cols), jnp.float32),
            pltpu.VMEM((2, 4, TAIL, LANES), jnp.bfloat16),
            pltpu.VMEM((2, block, LANES), jnp.float32),
            pltpu.SemaphoreType.DMA((3, max(9, len(weights)))),
        ],
        compiler_params=room(24),
        name="up_hidden",
    )(place, *near, *far, *weights, taps)


def project_kernel(place, heads, weights, keep, send, left, right, made, came, went, *, quarter):
    core = place[1] % 2
    count = right.shape[0]
    wide = right.shape[2]
    loads = [pltpu.make_async_copy(heads, left, came.at[count])]
    for n in range(count):
        cols = pl.ds(n * wide, wide)
        loads.append(pltpu.make_async_copy(weights.at[:, cols], right.at[n], came.at[n]))
    for copy in loads:
        copy.start()
    loads[0].wait()
    stores = []
    for n in range(count):
        loads[1 + n].wait()
        term = jnp.dot(left[...], right[n], preferred_element_type=jnp.float32)
        made[n] = term.astype(made.dtype)
        for f, (out, owner) in enumerate(((send, 1 - core), (keep, core))):
            for x in range(2):
                start = pl.multiple_of((2 * x + owner) * quarter, quarter)
                copy = pltpu.make_async_copy(
                    made.at[n, pl.ds(start, quarter + TAIL)],
                    out.at[x, :, pl.ds(n * wide, wide)],
                    went.at[n, 2 * f + x],
                )
                copy.start()
                stores.append(copy)
    for copy in stores:
        copy.wait()


def project(place, heads, weights, quarter):
    count, rows = 4, heads.shape[0]
    depth, width = weights.shape
    shape = jax.ShapeDtypeStruct((2, quarter + TAIL, width), jnp.bfloat16)
    anywhere = pl.BlockSpec(memory_space=pl.ANY)
    return pl.pallas_call(
        functools.partial(project_kernel, quarter=quarter),
        in_specs=[pl.BlockSpec(memory_space=pltpu.SMEM), anywhere, anywhere],
        out_specs=[anywhere, anywhere],
        out_shape=[shape, shape],
        scratch_shapes=[
            pltpu.VMEM((rows, depth), jnp.bfloat16),
            pltpu.VMEM((count, depth, width // count), jnp.bfloat16),
            pltpu.VMEM((count, rows, width // count), jnp.bfloat16),
            pltpu.SemaphoreType.DMA((count + 1,)),
            pltpu.SemaphoreType.DMA((count, 4)),
        ],
        compiler_params=room(RS_ROOM),
        name="project",
    )(place, heads, weights)


def merge_kernel(which, first, second, keep, send):
    own = which[0]
    for out, part in ((send, 1 - own), (keep, own)):
        out[...] = first[part] + second[part]


def merge(which, first, second):
    shape = jax.ShapeDtypeStruct(first.shape[1:], jnp.bfloat16)
    return pl.pallas_call(
        merge_kernel,
        in_specs=[pl.BlockSpec(memory_space=pltpu.SMEM), vmem(), vmem()],
        out_specs=[vmem(), vmem()],
        out_shape=[shape, shape],
        compiler_params=room(RS_ROOM),
        name="merge",
    )(which, first, second)


def fold_kernel(which, first, second, keep_a, send_a, keep_b, send_b):
    own = which[0]
    half = first.shape[3] // 2
    for l in range(2):
        for out, part in ((send_a, 1 - own), (keep_a, own)):
            out[l] = first[part, l, :, :half] + second[part, l, :, :half]
    for x in range(2):
        for out, part in ((send_b, 1), (keep_b, 0)):
            out[x] = first[x, part, :, half:] + second[x, part, :, half:]


def fold(which, first, second):
    _, _, rows, cols = first.shape
    shape = jax.ShapeDtypeStruct((2, rows, cols // 2), jnp.bfloat16)
    return pl.pallas_call(
        fold_kernel,
        in_specs=[pl.BlockSpec(memory_space=pltpu.SMEM), vmem(), vmem()],
        out_specs=[vmem()] * 4,
        out_shape=[shape] * 4,
        compiler_params=room(4),
        name="fold",
    )(which, first, second)


def refold_kernel(which, keep_a, came_a, keep_b, came_b, stay_a, send_a, stay_b, send_b):
    own = which[0]
    stay_a[...] = keep_a[0] + came_a[0]
    send_a[...] = keep_a[1] + came_a[1]
    stay_b[...] = keep_b[own] + came_b[own]
    send_b[...] = keep_b[1 - own] + came_b[1 - own]


def refold(which, *arrays):
    shape = jax.ShapeDtypeStruct(arrays[0].shape[1:], jnp.bfloat16)
    return pl.pallas_call(
        refold_kernel,
        in_specs=[pl.BlockSpec(memory_space=pltpu.SMEM)] + [vmem()] * 4,
        out_specs=[vmem()] * 4,
        out_shape=[shape] * 4,
        compiler_params=room(4),
        name="refold",
    )(which, *arrays)


def norm_kernel(place, first, second, residual, before, gain, flags, out, base, sems):
    tp = place[1]
    rows = first.shape[0]
    quarter = rows - TAIL
    start = pl.multiple_of(tp * quarter, quarter)
    body = pltpu.make_async_copy(
        residual.at[pl.ds(start, quarter)], base.at[pl.ds(TAIL, quarter)], sems.at[0]
    )
    body.start()
    top = base.at[pl.ds(0, TAIL)]

    @pl.when(tp == 0)
    def _():
        pltpu.make_async_copy(before, top, sems.at[1]).start()

    @pl.when(tp != 0)
    def _():
        at = pl.multiple_of(jnp.maximum(start - TAIL, 0), TAIL)
        pltpu.make_async_copy(residual.at[pl.ds(at, TAIL)], top, sems.at[1]).start()

    pltpu.make_async_copy(before, top, sems.at[1]).wait()
    body.wait()
    group = 64
    for r in range(0, rows, group):
        at = slice(r, min(r + group, rows))
        total = first[at].astype(jnp.float32) + second[at].astype(jnp.float32)
        total = mix_scale * base[at].astype(jnp.float32) + total
        mean = jnp.mean(total, axis=1, keepdims=True)
        total = total - mean
        var = jnp.mean(total * total, axis=1, keepdims=True)
        out[at] = (total * lax.rsqrt(var + norm_eps) * gain[...]).astype(out.dtype)
    line = lax.broadcasted_iota(jnp.int32, (TAIL, LANES), 0)
    rows_of = out[:TAIL, :LANES].astype(jnp.float32)
    out[:TAIL, :LANES] = jnp.where(line < 2, flags[...], rows_of).astype(out.dtype)


def normed_rows(place, first, second, residual, before, gain, flags):
    return pl.pallas_call(
        norm_kernel,
        in_specs=[pl.BlockSpec(memory_space=pltpu.SMEM), vmem(), vmem(), hbm(), hbm(), vmem(), vmem()],
        out_specs=vmem(),
        out_shape=jax.ShapeDtypeStruct(first.shape, jnp.bfloat16),
        scratch_shapes=[pltpu.VMEM(first.shape, jnp.bfloat16), pltpu.SemaphoreType.DMA((2,))],
        compiler_params=room(RS_ROOM),
        name="normed_rows",
    )(place, first, second, residual, before, gain, flags)


def down_kernel(place, near, far, *refs):
    *pieces, keep, send, ws, sems = refs
    if len(pieces) == 3:
        pieces.append(None)
    sp, tp = place[0], place[1]
    low, high, core = (sp // 2) % 2, sp // 4, tp % 2
    width = pieces[0].shape[1]
    copies = []
    for k, piece in enumerate(pieces):
        slot = 2 * (low ^ (k % 2) ^ core) + (high ^ (k // 2))
        dst = ws.at[:, pl.ds(pl.multiple_of(slot * width, width), width)]
        if piece is not None:
            copies.append(pltpu.make_async_copy(piece, dst, sems.at[k]))
            copies[-1].start()
        else:
            ws[:, pl.ds(pl.multiple_of(slot * width, width), width)] = jnp.zeros(
                (ws.shape[0], width), ws.dtype
            )
    for copy in copies:
        copy.wait()
    for out, base in ((send, 2 * width), (keep, 0)):
        for m, hidden in enumerate((near, far)):
            term = jnp.dot(
                hidden[...], ws[:, base : base + 2 * width], preferred_element_type=jnp.float32
            )
            for owner_x in range(2):
                out[owner_x, m] = term[:, owner_x * width : (owner_x + 1) * width].astype(out.dtype)


def down_terms(place, near, far, pieces):
    shape = (2, 2, near.shape[0], pieces[0].shape[1])
    shape = jax.ShapeDtypeStruct(shape, jnp.bfloat16)
    anywhere = pl.BlockSpec(memory_space=pl.ANY)
    return pl.pallas_call(
        down_kernel,
        in_specs=[pl.BlockSpec(memory_space=pltpu.SMEM), vmem(), vmem()] + [anywhere] * len(pieces),
        out_specs=[vmem(), vmem()],
        out_shape=[shape, shape],
        scratch_shapes=[
            pltpu.VMEM((pieces[0].shape[0], 4 * pieces[0].shape[1]), jnp.bfloat16),
            pltpu.SemaphoreType.DMA((4,)),
        ],
        compiler_params=room(12),
        name="down_terms",
    )(place, near, far, *pieces)


def last_kernel(place, near, far, piece, keep_in, send_in, keep, send, made, sems):
    sp, tp = place[0], place[1]
    low, high, core = (sp // 2) % 2, sp // 4, tp % 2
    for m, hidden in enumerate((near, far)):
        term = jnp.dot(hidden[...], piece[...], preferred_element_type=jnp.float32)
        made[m] = term.astype(made.dtype)
    leaves = low ^ core ^ 1

    @pl.when(leaves == 0)
    def _():
        pltpu.make_async_copy(made, keep.at[1 - high], sems.at[0]).start()

    @pl.when(leaves != 0)
    def _():
        pltpu.make_async_copy(made, send.at[1 - high], sems.at[0]).start()

    pltpu.make_async_copy(made, keep.at[1 - high], sems.at[0]).wait()


def last_terms(place, near, far, piece, keep, send):
    shape = jax.ShapeDtypeStruct(keep.shape, keep.dtype)
    anywhere = pl.BlockSpec(memory_space=pl.ANY)
    return pl.pallas_call(
        last_kernel,
        in_specs=[pl.BlockSpec(memory_space=pltpu.SMEM)] + [vmem()] * 3 + [anywhere] * 2,
        out_specs=[anywhere] * 2,
        out_shape=[shape, shape],
        scratch_shapes=[
            pltpu.VMEM(keep.shape[1:], keep.dtype),
            pltpu.SemaphoreType.DMA((1,)),
        ],
        input_output_aliases={4: 0, 5: 1},
        compiler_params=room(8),
        name="last_terms",
    )(place, near, far, piece, keep, send)


def reduced(keep, send, x):
    came = swapped(send, tp_mask=1)
    keep_a, send_a, keep_b, send_b = fold(x, keep, came)
    came_b = swapped(send_b, sp_mask=2)
    came_a = swapped(send_a, tp_mask=2)
    keep_a, send_a, keep_b, send_b = refold(x, keep_a, came_a, keep_b, came_b)
    came_a = swapped(send_a, sp_mask=2)
    came_b = swapped(send_b, tp_mask=2)
    add = lambda one, two: one.astype(jnp.float32) + two.astype(jnp.float32)
    return jnp.concatenate([add(keep_a, came_a), add(keep_b, came_b)], axis=1)


def local_heads(came, query_rows, key_rows, value_rows, doc_ids, sink_logit):
    rows = query_rows.shape[0]
    kv_local = key_rows.shape[1] // HD
    heads_local = query_rows.shape[1] // HD
    groups = heads_local // kv_local
    reach = WIN + TAIL
    offset = lax.axis_index("sp") * rows
    at = 4 * HD * WIN // LANES
    wide = lambda lines: jnp.concatenate(
        [lines[i : i + TAIL] for i in range(0, lines.shape[0], TAIL)], axis=1
    )
    q_lines = TAIL * query_rows.shape[1] // LANES
    prev_keys, prev_values = (
        jnp.concatenate([came[i : i + HD], came[i + HD : i + 2 * HD]], axis=1)[:, 2 * WIN - reach :]
        for i in (0, 2 * HD)
    )
    prev_docs = came[at : at + 2].reshape(2 * LANES)[2 * LANES - reach :].astype(jnp.int32)
    at = at + TAIL
    prev_queries = wide(came[at : at + q_lines])
    prev_residual = wide(came[at + q_lines :])
    all_keys = jnp.concatenate([prev_keys, key_rows.T], axis=1).T.reshape(rows + reach, kv_local, HD)
    all_values = jnp.concatenate([prev_values, value_rows.T], axis=1).T
    all_values = all_values.reshape(rows + reach, kv_local, HD)
    all_docs = jnp.concatenate([prev_docs, doc_ids])
    key_pos = offset - reach + jnp.arange(rows + reach, dtype=jnp.int32)
    query_pos = offset - TAIL + jnp.arange(rows + TAIL, dtype=jnp.int32)
    queries = jnp.concatenate([prev_queries, query_rows]).reshape(rows + TAIL, kv_local, groups, HD)
    sink = sink_logit.reshape(kv_local, groups, 1, 1)
    pieces = attend(
        queries, all_keys, all_values, query_pos, key_pos, all_docs[WIN:], all_docs, sink
    )
    return pieces.reshape(rows + TAIL, heads_local * HD), prev_docs, prev_residual


def paired(
    query_rows,
    key_rows,
    value_rows,
    doc_ids,
    sink_logit,
    residual,
    out_proj,
    mix_gain,
    gate_proj,
    value_proj,
    gate_taps,
    value_taps,
    down_proj,
    final_gain,
):
    rows, width = residual.shape
    n_tp = lax.axis_size("tp")
    quarter = rows // n_tp
    share = width // n_tp
    sp, tp = lax.axis_index("sp"), lax.axis_index("tp")
    y, low = sp % 2, (sp // 2) % 2
    x, core = tp // 2, tp % 2
    place = jnp.stack([sp, tp]).astype(jnp.int32)
    one = lambda index: index.astype(jnp.int32)[None]
    low_at, x_at, core_at = one(low), one(x), one(core)

    docs_rows = doc_ids.reshape(rows // LANES, LANES)
    halo = packed(query_rows, key_rows, value_rows, docs_rows, residual)
    came_halo = passed_along(halo, "sp", 1)
    own, other = prepared(low_at, gate_proj, value_proj)
    from_z = [own, swapped(other, 2), swapped(own, 4), swapped(other, 6)]
    up_weights = []
    for piece in from_z:
        up_weights += [piece, swapped(piece, 1)]
    own, other = row_halves(low_at, down_proj)
    down_same = [own, swapped(other, 2), swapped(own, 4), swapped(other, 6)]
    down_far = [swapped(piece, 1) for piece in down_same]

    heads, prev_docs, prev_residual = local_heads(
        came_halo, query_rows, key_rows, value_rows, doc_ids, sink_logit
    )
    docs = jnp.concatenate([prev_docs[-2:], doc_ids])
    flags = jnp.stack([docs[1:-1] == doc_ids, docs[:-2] == doc_ids]).astype(jnp.float32)
    flags = lax.dynamic_slice_in_dim(flags, tp * quarter, quarter, 1)
    flags = jnp.pad(flags, ((0, TAIL - 2), (0, 0)))
    keep, send = project(place, heads, out_proj, quarter)
    came = swapped(send, tp_mask=1)
    keep, send = merge(x_at, keep, came)
    came = swapped(send, tp_mask=2)
    normed = normed_rows(
        place, keep, came, residual, prev_residual, mix_gain[None, :], flags
    )
    near = [normed, swapped(normed, tp_mask=2)]
    near += [swapped(near[0], tp_mask=1), swapped(near[1], tp_mask=1)]
    normed = swapped(normed, sp_mask=2)
    far = [normed, swapped(normed, tp_mask=2)]
    far += [swapped(far[0], tp_mask=1), swapped(far[1], tp_mask=1)]

    cols = gate_proj.shape[1]
    half = cols // 2
    main = half // LANES * LANES
    rest = half - main
    cut = lambda taps, start, size: lax.dynamic_slice_in_dim(taps, start, size, 1)
    mains = [cut(t, low * (cols - main), main) for t in (gate_taps, value_taps)]
    rests = [cut(t, main + low * rest, rest) for t in (gate_taps, value_taps)]
    mains = jnp.stack([t.reshape(TAPS, main // LANES, LANES) for t in mains], axis=2)
    taps = jnp.concatenate([mains.reshape(TAPS, 2 * main), *rests], axis=1)
    taps = jnp.pad(taps, ((0, 8 - TAPS), (0, 0)))

    near, far, own_normed = up_hidden(place, near, far, up_weights, taps, share)
    terms = down_terms(place, near, far, down_same)
    ffn_same = reduced(*terms, x_at)
    terms = down_terms(place, near, far, down_far[:3])
    terms = last_terms(place, near, far, down_far[3], *terms)
    ffn_far = reduced(*terms, x_at)
    ffn_own = jnp.where(
        y == 0,
        jnp.concatenate([ffn_same, ffn_far], axis=1),
        jnp.concatenate([ffn_far, ffn_same], axis=1),
    )
    second_sum = mix_scale * own_normed.astype(jnp.float32) + ffn_own
    row_sum, row_squares = lax.psum(
        (jnp.sum(second_sum, axis=1), jnp.sum(second_sum * second_sum, axis=1)), "tp"
    )
    mean = row_sum / width
    var = jnp.maximum(row_squares / width - mean * mean, 0.0)
    return (
        (second_sum - mean[:, None]) * lax.rsqrt(var + norm_eps)[:, None] * final_gain[None, :]
    ).astype(jnp.bfloat16)


def on_device(
    query_rows,
    key_rows,
    value_rows,
    doc_ids,
    sink_logit,
    residual,
    out_proj,
    mix_gain,
    gate_proj,
    value_proj,
    gate_taps,
    value_taps,
    down_proj,
    final_gain,
):
    rows = query_rows.shape[0]
    kv_local = key_rows.shape[1] // HD
    heads_local = query_rows.shape[1] // HD
    groups = heads_local // kv_local
    offset = lax.axis_index("sp") * rows
    prev_keys, prev_values, prev_docs = passed_along(
        (key_rows[rows - WIN :], value_rows[rows - WIN :], doc_ids[rows - WIN :]), "sp", 1
    )
    all_keys = jnp.concatenate([prev_keys, key_rows]).reshape(rows + WIN, kv_local, HD)
    all_values = jnp.concatenate([prev_values, value_rows]).reshape(rows + WIN, kv_local, HD)
    all_docs = jnp.concatenate([prev_docs, doc_ids])
    key_pos = offset - WIN + jnp.arange(rows + WIN, dtype=jnp.int32)
    query_pos = offset + jnp.arange(rows, dtype=jnp.int32)
    queries = query_rows.reshape(rows, kv_local, groups, HD)
    sink = sink_logit.reshape(kv_local, groups, 1, 1)
    pieces = attend(queries, all_keys, all_values, query_pos, key_pos, doc_ids, all_docs, sink)
    heads = pieces.reshape(rows, heads_local * HD)
    partial_value = jnp.dot(heads, out_proj, preferred_element_type=jnp.float32)
    width = residual.shape[1]
    share = width // lax.axis_size("tp")
    col_start = lax.axis_index("tp") * share
    attn_total = lax.psum(partial_value.astype(jnp.bfloat16), "tp").astype(jnp.float32)
    first_sum = mix_scale * residual.astype(jnp.float32) + attn_total
    mean = jnp.mean(first_sum, axis=1, keepdims=True)
    var = jnp.mean(jnp.square(first_sum - mean), axis=1, keepdims=True)
    normed = ((first_sum - mean) * lax.rsqrt(var + norm_eps) * mix_gain[None, :]).astype(
        jnp.bfloat16
    )
    normed_own = lax.dynamic_slice_in_dim(normed, col_start, share, 1)
    up_gate = jnp.dot(
        normed,
        lax.all_gather(gate_proj, "sp", axis=0, tiled=True),
        preferred_element_type=jnp.float32,
    )
    up_value = jnp.dot(
        normed,
        lax.all_gather(value_proj, "sp", axis=0, tiled=True),
        preferred_element_type=jnp.float32,
    )
    up_gate = up_gate.astype(jnp.bfloat16)
    up_value = up_value.astype(jnp.bfloat16)
    lag_rows = TAPS - 1
    prev_gate, prev_value = passed_along(
        (up_gate[rows - lag_rows :], up_value[rows - lag_rows :]), "sp", 1
    )
    tail_docs = prev_docs[WIN - lag_rows :]
    conv_gate = depthwise(prev_gate, up_gate, gate_taps, tail_docs, doc_ids)
    conv_value = depthwise(prev_value, up_value, value_taps, tail_docs, doc_ids)
    hidden = (jax.nn.gelu(conv_gate) * conv_value).astype(jnp.bfloat16)
    terms = jnp.dot(
        hidden,
        lax.all_gather(down_proj, "sp", axis=1, tiled=True),
        preferred_element_type=jnp.float32,
    )
    ffn_own = lax.psum_scatter(
        terms.astype(jnp.bfloat16), "tp", scatter_dimension=1, tiled=True
    ).astype(jnp.float32)
    second_sum = mix_scale * normed_own.astype(jnp.float32) + ffn_own
    row_sum, row_squares = lax.psum(
        (jnp.sum(second_sum, axis=1), jnp.sum(second_sum * second_sum, axis=1)), "tp"
    )
    mean = row_sum / width
    var = row_squares / width - mean * mean
    return (
        (second_sum - mean[:, None]) * lax.rsqrt(var + norm_eps)[:, None] * final_gain[None, :]
    ).astype(jnp.bfloat16)


def solution(mesh):
    placed = (
        P("sp", "tp"),
        P("sp", "tp"),
        P("sp", "tp"),
        P("sp"),
        P("tp"),
        P("sp", None),
        P("tp", None),
        P(),
        P("sp", "tp"),
        P("sp", "tp"),
        P(None, "tp"),
        P(None, "tp"),
        P("tp", "sp"),
        P("tp"),
    )
    fits = mesh.shape["sp"] == 2 * mesh.shape["tp"] and mesh.shape["tp"] == 4
    return jax.shard_map(
        paired if fits else on_device,
        mesh=mesh,
        in_specs=placed,
        out_specs=P("sp", "tp"),
        check_vma=False,
    )
```
